768 devices in a mesh: ep: 48 (over z, x), tp: 16 (over y, core).
Axes of the slice: x: 4, y: 8, z: 12, core: 2. Of those that a mesh axis runs over, the one named last changes fastest.
Arguments:
- stream: bfloat16 [960, 2048], P('ep'), may hold values from -8 to 8
- norm_gain_mix: bfloat16 [2048], replicated, may hold values from 0.099609375 to 1.8984375
- query_weight: bfloat16 [1024, 2048], P('tp'), may hold values from -0.125 to 0.125
- key_weight: bfloat16 [1024, 2048], P('tp'), may hold values from -0.125 to 0.125
- value_weight: bfloat16 [1024, 2048], P('tp'), may hold values from -0.125 to 0.125
- score_offset: float32 [16], P('tp'), may hold values from -9 to -3
- cache_keys: bfloat16 [960, 1024, 256], P('ep', 'tp'), may hold values from -6 to 6
- cache_values: bfloat16 [960, 1024, 256], P('ep', 'tp'), may hold values from -6 to 6
- lengths: int32 [960], P('ep'), may hold values from 32 to 256, as said below
- out_weight: bfloat16 [1024, 2048], P('tp'), may hold values from -0.75 to 0.75
- norm_gain_ffn: bfloat16 [2048], replicated, may hold values from 0.099609375 to 1.8984375
- group_weight: bfloat16 [2048, 4], replicated, may hold values from -0.25 to 0.25
- router_weight: bfloat16 [2048, 48], replicated, may hold values from -0.25 to 0.25
- routing: int32 [960, 2], P('ep'), may hold values from 0 to 47, as said below
- expert_gate: bfloat16 [48, 2048, 4096], P('ep', None, 'tp'), may hold values from -0.125 to 0.125
- expert_up: bfloat16 [48, 2048, 4096], P('ep', None, 'tp'), may hold values from -0.125 to 0.125
- expert_down: bfloat16 [48, 4096, 2048], P('ep', 'tp'), may hold values from -0.1875 to 0.1875
- branch_gate: bfloat16 [2048], replicated, may hold values from -0.25 to 0.25
- dense_gate: bfloat16 [2048, 6144], P('tp', 'ep'), may hold values from -0.125 to 0.125
- dense_up: bfloat16 [2048, 6144], P('tp', 'ep'), may hold values from -0.125 to 0.125
- dense_down: bfloat16 [6144, 2048], P('ep', 'tp'), may hold values from -0.15625 to 0.15625
Outputs:
- mixed: bfloat16 [960, 2048], P('ep', 'tp')
- fresh_keys: bfloat16 [960, 1024], P('ep', 'tp')
- fresh_values: bfloat16 [960, 1024], P('ep', 'tp')
The draws below stay inside these ranges and needn't reach their ends.
Inputs may be any that keep to these rules, and one draw needn't show every extreme that they name: `routing`: each aligned block of 20 rows (the sequences of one index of ep) names no expert more than 2 times, and some expert exactly 2 times; a row's two experts differ and lie in the same group of 12 consecutive experts. `lengths`: in every aligned block of 20 sequences one sequence has all 256 positions filled.
All inputs are finite; a program needn't handle non-finite values.
Results may differ from the reference program's by a relative error of at most 0.02.
Values may be sent and summed in bfloat16 or wider, within the bound.
No kernel may reach another device: no remote copies, remote signals or barrier semaphores. Data moves between devices by JAX's collectives and lax.ppermute only.
A program may use at most 64 MiB of HBM per device.

```python
import jax
import jax.numpy as jnp
from jax import lax

WIDTH = 2048
HEADS = 16
HEAD_DIM = 64
GROUPS = 4
FF_EXP = 4096
FF_DENSE = 6144
TOP_K = 2
SEQ_DEV = 20
CACHE = 256
KV_WIDTH = 1024
EXPERTS = 48
CAP = 2
SEQS = 960
N_EP = 48
N_TP = 16


def draw_stream(key, part):
    columns = jnp.arange(WIDTH, dtype=jnp.float32) / WIDTH
    base = jnp.clip(jax.random.normal(key, (SEQS, WIDTH), jnp.float32), -4.0, 4.0)
    return (base * (0.6 * 3.0 ** columns)[None, :]).astype(jnp.bfloat16)


def draw_score_offset(key, part):
    return jax.random.uniform(key, (HEADS,), jnp.float32, -9.0, -3.0)


def draw_lengths(key, part):
    filled = jax.random.randint(key, (SEQS,), CACHE // 8, CACHE + 1)
    chosen = jax.random.randint(jax.random.fold_in(key, 1), (SEQS // SEQ_DEV,), 0, SEQ_DEV)
    within = jnp.arange(SEQS, dtype=jnp.int32).reshape(SEQS // SEQ_DEV, SEQ_DEV) % SEQ_DEV
    full = (within == chosen[:, None]).reshape(SEQS)
    return jnp.where(full, CACHE, filled).astype(jnp.int32)


def route_block(key):
    rounds = (SEQ_DEV + EXPERTS - 1) // EXPERTS
    per_group = EXPERTS // GROUPS
    firsts = []
    seconds = []
    for which in range(rounds):
        order = jax.random.permutation(jax.random.fold_in(key, 2 * which), EXPERTS).astype(jnp.int32)
        offset = jax.random.randint(jax.random.fold_in(key, 2 * which + 1), (), 0, per_group - 1)
        target = order[0] // per_group * per_group + (order[0] % per_group + 1 + offset) % per_group
        where_at = jnp.argmax(order == target)
        order = order.at[where_at].set(order[1]).at[1].set(target)
        partner = order // per_group * per_group + (order % per_group + 1 + offset) % per_group
        firsts.append(order)
        seconds.append(partner)
    first = jnp.concatenate(firsts)[:SEQ_DEV]
    second = jnp.concatenate(seconds)[:SEQ_DEV]
    paired = jnp.stack([first, second], 1)
    flipped = jax.random.randint(jax.random.fold_in(key, 1000), (SEQ_DEV, 1), 0, 2)
    paired = jnp.where(flipped == 1, paired[:, ::-1], paired)
    shuffle = jax.random.permutation(jax.random.fold_in(key, 1001), SEQ_DEV)
    return paired[shuffle].astype(jnp.int32)


def draw_routing(key, part):
    numbers = jnp.arange(SEQS // SEQ_DEV, dtype=jnp.int32)
    routed = jax.vmap(lambda number: route_block(jax.random.fold_in(key, number)))(numbers)
    return routed.reshape(SEQS, TOP_K).astype(jnp.int32)


def levels(rng, dims, cuts, least, high):
    level, own = 1.0, jax.random.fold_in(rng, 6)
    for dim, shards_of in cuts:
        heights = jnp.exp(jax.random.uniform(jax.random.fold_in(own, dim), (shards_of,), jnp.float32, least / len(cuts), high / len(cuts)))
        level = level * jnp.repeat(heights, dims[dim] // shards_of).reshape([-1 if axis == dim else 1 for axis in range(len(dims))])
    return level


def centred(key, shape, width, most, cuts=(), held_as=jnp.bfloat16):
    level = levels(key, shape, cuts, -0.22, 0.18) if cuts else 1.0
    result = jax.random.normal(key, shape, jnp.float32) * width * level
    return jnp.minimum(jnp.maximum(result, -most), most).astype(held_as)


def setup_inputs(seed: int = 0) -> dict:
    splits = jax.random.split(jax.random.key(seed), 22)
    return {
        "stream": draw_stream(jax.random.fold_in(splits[21], 71), 0),
        "norm_gain_mix": jnp.clip(1.0 + 0.18 * jax.random.normal(splits[1], (WIDTH,), jnp.float32), 0.099609375, 1.8984375).astype(jnp.bfloat16),
        "query_weight": centred(splits[2], (KV_WIDTH, WIDTH), WIDTH ** -0.5, 0.125, ((0, 16),)),
        "key_weight": centred(splits[3], (KV_WIDTH, WIDTH), WIDTH ** -0.5, 0.125, ((0, 16),)),
        "value_weight": centred(splits[4], (KV_WIDTH, WIDTH), WIDTH ** -0.5, 0.125, ((0, 16),)),
        "score_offset": draw_score_offset(jax.random.fold_in(splits[21], 71), 0),
        "cache_keys": centred(splits[6], (SEQS, KV_WIDTH, CACHE), 1.0, 6.0, ((0, 48), (1, 16))),
        "cache_values": centred(splits[7], (SEQS, KV_WIDTH, CACHE), 1.0, 6.0, ((0, 48), (1, 16))),
        "lengths": draw_lengths(jax.random.fold_in(splits[21], 71), 0),
        "out_weight": centred(splits[9], (KV_WIDTH, WIDTH), HEAD_DIM ** -0.5, 0.75, ((0, 16),)),
        "norm_gain_ffn": jnp.clip(1.0 + 0.18 * jax.random.normal(splits[10], (WIDTH,), jnp.float32), 0.099609375, 1.8984375).astype(jnp.bfloat16),
        "group_weight": centred(splits[11], (WIDTH, GROUPS), (WIDTH // 4) ** -0.5, 0.25),
        "router_weight": centred(splits[12], (WIDTH, EXPERTS), (WIDTH // 4) ** -0.5, 0.25),
        "routing": draw_routing(jax.random.fold_in(splits[21], 71), 0),
        "expert_gate": centred(splits[14], (EXPERTS, WIDTH, FF_EXP), WIDTH ** -0.5, 0.125, ((0, 48), (2, 16))),
        "expert_up": centred(splits[15], (EXPERTS, WIDTH, FF_EXP), WIDTH ** -0.5, 0.125, ((0, 48), (2, 16))),
        "expert_down": centred(splits[16], (EXPERTS, FF_EXP, WIDTH), (FF_EXP // 4) ** -0.5, 0.1875, ((0, 48), (1, 16))),
        "branch_gate": centred(splits[17], (WIDTH,), (WIDTH // 4) ** -0.5, 0.25),
        "dense_gate": centred(splits[18], (WIDTH, FF_DENSE), WIDTH ** -0.5, 0.125, ((0, 16), (1, 48))),
        "dense_up": centred(splits[19], (WIDTH, FF_DENSE), WIDTH ** -0.5, 0.125, ((0, 16), (1, 48))),
        "dense_down": centred(splits[20], (FF_DENSE, WIDTH), (FF_DENSE // 4) ** -0.5, 0.15625, ((0, 48), (1, 16))),
    }


epsilon = 1e-06

def rounded(value):
    return lax.optimization_barrier(value.astype(jnp.bfloat16)).astype(jnp.float32)

def project_rows(normed, weight):
    return lax.dot_general(normed, weight, (((1,), (1,)), ((), ())), preferred_element_type=jnp.float32)

def stick_weights(scores, inside):
    log_keep = jnp.where(inside, jax.nn.log_sigmoid(-scores), 0.0)
    remain = lax.cumsum(log_keep, axis=2, reverse=True) - log_keep
    return jnp.where(inside, jnp.exp(jax.nn.log_sigmoid(scores) + remain), 0.0)

def reference(stream, norm_gain_mix, query_weight, key_weight, value_weight, score_offset, cache_keys, cache_values, lengths, out_weight, norm_gain_ffn, group_weight, router_weight, routing, expert_gate, expert_up, expert_down, branch_gate, dense_gate, dense_up, dense_down):
    blocks = N_EP
    stream_f = stream.astype(jnp.float32)
    inverse = lax.rsqrt(lax.optimization_barrier(jnp.mean(stream_f * stream_f, -1, keepdims=True)) + epsilon)
    normed = (stream_f * inverse * norm_gain_mix.astype(jnp.float32)).astype(jnp.bfloat16)
    queries = project_rows(normed, query_weight).astype(jnp.bfloat16)
    fresh_keys = project_rows(normed, key_weight).astype(jnp.bfloat16)
    fresh_values = project_rows(normed, value_weight).astype(jnp.bfloat16)

    def attend(inputs):
        block_q, block_k, block_v, block_len = inputs
        query_h = block_q.reshape(SEQ_DEV, HEADS, HEAD_DIM).astype(jnp.float32)
        key_h = block_k.reshape(SEQ_DEV, HEADS, HEAD_DIM, CACHE).astype(jnp.float32)
        value_h = block_v.reshape(SEQ_DEV, HEADS, HEAD_DIM, CACHE).astype(jnp.float32)
        scores = jnp.einsum('shd,shdl->shl', query_h, key_h) * HEAD_DIM ** (-0.5) + score_offset[None, :, None]
        inside = jnp.arange(CACHE, dtype=jnp.int32)[None, None, :] < block_len[:, None, None]
        weights = stick_weights(scores, inside).astype(jnp.bfloat16)
        mixed_h = jnp.einsum('shl,shdl->shd', weights.astype(jnp.float32), value_h)
        return mixed_h.astype(jnp.bfloat16).reshape(SEQ_DEV, KV_WIDTH)
    heads_out = lax.map(attend, (queries.reshape(blocks, SEQ_DEV, KV_WIDTH), cache_keys.reshape(blocks, SEQ_DEV, KV_WIDTH, CACHE), cache_values.reshape(blocks, SEQ_DEV, KV_WIDTH, CACHE), lengths.reshape(blocks, SEQ_DEV))).reshape(SEQS, KV_WIDTH)
    span = KV_WIDTH // N_TP
    attn_total = jnp.zeros((SEQS, WIDTH), jnp.float32)
    for index_tp in range(N_TP):
        attn_total = attn_total + rounded(jnp.dot(heads_out[:, index_tp * span:(index_tp + 1) * span], out_weight[index_tp * span:(index_tp + 1) * span], preferred_element_type=jnp.float32))
    attn = attn_total.astype(jnp.bfloat16)
    residual = (stream_f + attn.astype(jnp.float32)).astype(jnp.bfloat16)
    residual_f = residual.astype(jnp.float32)
    inverse_two = lax.rsqrt(lax.optimization_barrier(jnp.mean(residual_f * residual_f, -1)) + epsilon)
    group_logits = jnp.dot(residual, group_weight, preferred_element_type=jnp.float32) * inverse_two[:, None]
    expert_logits = jnp.dot(residual, router_weight, preferred_element_type=jnp.float32) * inverse_two[:, None]
    gate_logit = jnp.dot(residual, branch_gate, preferred_element_type=jnp.float32) * inverse_two
    hidden_in = (residual_f * inverse_two[:, None] * norm_gain_ffn.astype(jnp.float32)).astype(jnp.bfloat16)
    per_group = EXPERTS // GROUPS
    group_index = routing[:, 0] // per_group
    group_exp = jnp.exp(group_logits)
    own_group = jnp.take_along_axis(group_exp, group_index[:, None], 1)[:, 0]
    group_prob = own_group / lax.optimization_barrier(jnp.sum(group_exp, -1))
    chosen_exp = jnp.exp(jnp.take_along_axis(expert_logits, routing, 1))
    route_gate = group_prob[:, None] * chosen_exp / lax.optimization_barrier(jnp.sum(chosen_exp, -1, keepdims=True))
    pairs = routing.reshape(blocks, SEQ_DEV * TOP_K)
    onehot = (pairs[:, :, None] == jnp.arange(EXPERTS, dtype=jnp.int32)[None, None, :]).astype(jnp.int32)
    before = jnp.cumsum(onehot, 1) - onehot
    slot = lax.optimization_barrier(jnp.sum(before * onehot, -1))
    index = (pairs * CAP + slot).astype(jnp.int32)
    dispatch = (index[:, None, :] == jnp.arange(EXPERTS * CAP, dtype=jnp.int32)[None, :, None]).astype(jnp.float32)
    dispatch = lax.optimization_barrier(jnp.sum(dispatch.reshape(blocks, EXPERTS * CAP, SEQ_DEV, TOP_K), -1))
    rows = jnp.einsum('bjs,bsd->bjd', dispatch, hidden_in.reshape(blocks, SEQ_DEV, WIDTH).astype(jnp.float32))
    rows = rows.astype(jnp.bfloat16).reshape(blocks, EXPERTS, CAP, WIDTH)
    expert_rows = rows.transpose(1, 0, 2, 3).reshape(EXPERTS, blocks * CAP, WIDTH)
    span_ff = FF_EXP // N_TP

    def expert(inputs):
        block_rows, weight_gate, weight_up, weight_down = inputs
        gate_val = jnp.dot(block_rows, weight_gate, preferred_element_type=jnp.float32)
        up_val = jnp.dot(block_rows, weight_up, preferred_element_type=jnp.float32)
        hidden = (jax.nn.silu(gate_val) * up_val).astype(jnp.bfloat16)
        total = jnp.zeros((block_rows.shape[0], WIDTH), jnp.float32)
        for index_tp in range(N_TP):
            total = total + rounded(jnp.dot(hidden[:, index_tp * span_ff:(index_tp + 1) * span_ff], weight_down[index_tp * span_ff:(index_tp + 1) * span_ff], preferred_element_type=jnp.float32))
        return total.astype(jnp.bfloat16)
    expert_out = lax.map(expert, (expert_rows, expert_gate, expert_up, expert_down))
    back = expert_out.reshape(EXPERTS, blocks, CAP, WIDTH).transpose(1, 0, 2, 3).reshape(blocks, EXPERTS * CAP, WIDTH)
    where_rows = jnp.broadcast_to(index[:, :, None], (blocks, SEQ_DEV * TOP_K, WIDTH))
    picked = jnp.take_along_axis(back, where_rows, 1).astype(jnp.float32).reshape(SEQS, TOP_K, WIDTH)
    moe = lax.optimization_barrier(jnp.sum(route_gate[:, :, None] * picked, 1))
    span_feat = WIDTH // N_TP
    dense_g = jnp.zeros((SEQS, FF_DENSE), jnp.float32)
    dense_u = jnp.zeros((SEQS, FF_DENSE), jnp.float32)
    for index_tp in range(N_TP):
        piece = hidden_in[:, index_tp * span_feat:(index_tp + 1) * span_feat]
        dense_g = dense_g + rounded(jnp.dot(piece, dense_gate[index_tp * span_feat:(index_tp + 1) * span_feat], preferred_element_type=jnp.float32))
        dense_u = dense_u + rounded(jnp.dot(piece, dense_up[index_tp * span_feat:(index_tp + 1) * span_feat], preferred_element_type=jnp.float32))
    dense_act = (jax.nn.silu(dense_g) * dense_u).astype(jnp.bfloat16)
    dense = jnp.dot(dense_act, dense_down, preferred_element_type=jnp.float32)
    mixed = (residual_f + moe + jax.nn.sigmoid(gate_logit)[:, None] * dense).astype(jnp.bfloat16)
    return (mixed, fresh_keys, fresh_values)
```

```python
import jax
import jax.numpy as jnp
from jax import lax
from jax.sharding import PartitionSpec as P

epsilon = 1e-06


def project_rows(normed, weight):
    return lax.dot_general(
        normed, weight, (((1,), (1,)), ((), ())), preferred_element_type=jnp.float32
    )


def stick_weights(scores, inside):
    positions = scores.shape[1]
    log_keep = jnp.where(inside, jax.nn.log_sigmoid(-scores), 0.0)
    rows = lax.broadcasted_iota(jnp.int32, (positions, positions), 0)
    columns = lax.broadcasted_iota(jnp.int32, (positions, positions), 1)
    after = (rows > columns).astype(jnp.float32)
    remain = jnp.dot(
        log_keep, after, precision=lax.Precision.HIGHEST, preferred_element_type=jnp.float32
    )
    return jnp.where(inside, jnp.exp(jax.nn.log_sigmoid(scores) + remain), 0.0)


def exchange(array, axis):
    return lax.all_to_all(array, axis, 0, 0, tiled=True)


def to_pair(value):
    high = lax.reduce_precision(value, 8, 7)
    return high.astype(jnp.bfloat16), (value - high).astype(jnp.bfloat16)


def round_up(count, unit=8):
    return -(-count // unit) * unit


def sum_lead(array):
    return jnp.sum(array.astype(jnp.float32), axis=0)


def local(
    stream,
    norm_gain_mix,
    query_weight,
    key_weight,
    value_weight,
    score_offset,
    cache_keys,
    cache_values,
    lengths,
    out_weight,
    norm_gain_ffn,
    group_weight,
    router_weight,
    routing,
    expert_gate,
    expert_up,
    expert_down,
    branch_gate,
    dense_gate,
    dense_up,
    dense_down,
):
    seq_count = stream.shape[0]
    width = stream.shape[1]
    n_tp = lax.axis_size("tp")
    n_ep = lax.axis_size("ep")
    tp_rank = lax.axis_index("tp")
    feat = width // n_tp
    offset = tp_rank * feat
    rows_pad = round_up(seq_count)

    stream_f = stream.astype(jnp.float32)
    inverse = lax.rsqrt(jnp.mean(stream_f * stream_f, -1, keepdims=True) + epsilon)
    normed = (stream_f * inverse * norm_gain_mix.astype(jnp.float32)).astype(jnp.bfloat16)
    queries = project_rows(normed, query_weight).astype(jnp.bfloat16)
    fresh_keys = project_rows(normed, key_weight).astype(jnp.bfloat16)
    fresh_values = project_rows(normed, value_weight).astype(jnp.bfloat16)
    head_size = queries.shape[1]
    cache_len = cache_keys.shape[2]
    scores = jnp.einsum("sd,sdl->sl", queries, cache_keys, preferred_element_type=jnp.float32)
    scores = scores * head_size ** (-0.5) + score_offset[0]
    inside = lax.broadcasted_iota(jnp.int32, (1, cache_len), 1) < lengths[:, None]
    weights = stick_weights(scores, inside).astype(jnp.bfloat16)
    heads_out = jnp.einsum("sl,sdl->sd", weights, cache_values, preferred_element_type=jnp.float32)
    heads_out = jnp.pad(heads_out.astype(jnp.bfloat16), ((0, rows_pad - seq_count), (0, 0)))
    partial_value = jnp.dot(heads_out, out_weight, preferred_element_type=jnp.float32)
    terms = partial_value.astype(jnp.bfloat16).reshape(rows_pad, n_tp, feat)
    attn = sum_lead(exchange(jnp.moveaxis(terms, 1, 0), "tp"))[:seq_count]

    residual = (
        lax.dynamic_slice_in_dim(stream, offset, feat, 1).astype(jnp.float32)
        + attn.astype(jnp.bfloat16).astype(jnp.float32)
    ).astype(jnp.bfloat16)
    residual_own = residual.astype(jnp.float32)

    experts = router_weight.shape[1]
    groups = group_weight.shape[1]
    per_group = experts // groups
    top = routing.shape[1]
    cap = 2 * ((seq_count + experts - 1) // experts)
    expert_iota = lax.broadcasted_iota(jnp.int32, (1, experts), 1)
    pair_expert = routing.reshape(seq_count * top)
    onehot = (pair_expert[:, None] == expert_iota).astype(jnp.int32)
    before = jnp.cumsum(onehot, 0) - onehot
    slot = jnp.sum(before * onehot, 1)
    index = (pair_expert * cap + slot).reshape(seq_count, top)
    slot_iota = lax.broadcasted_iota(jnp.int32, (experts * cap, 1, 1), 0)
    dispatch = jnp.sum((index[None, :, :] == slot_iota).astype(jnp.int32), 2).astype(jnp.bfloat16)
    send = jnp.dot(dispatch, residual, preferred_element_type=jnp.float32).astype(jnp.bfloat16)

    both = seq_count + cap
    both_pad = round_up(both)
    arrived = exchange(
        jnp.concatenate(
            [
                jnp.broadcast_to(residual[None], (n_ep, seq_count, feat)),
                send.reshape(n_ep, cap, feat),
                jnp.zeros((n_ep, both_pad - both, feat), jnp.bfloat16),
            ],
            1,
        ),
        "ep",
    )
    total = n_ep * seq_count
    rows = arrived[:, :seq_count].reshape(total, feat).astype(jnp.float32)
    picked = arrived[:, seq_count:both].reshape(n_ep * cap, feat)

    home_weights = jnp.concatenate(
        [
            lax.dynamic_slice_in_dim(group_weight, offset, feat, 0),
            lax.dynamic_slice_in_dim(router_weight, offset, feat, 0),
            lax.dynamic_slice_in_dim(branch_gate, offset, feat, 0)[:, None],
        ],
        1,
    )
    products = jnp.dot(residual, home_weights, preferred_element_type=jnp.float32)
    expert_part = products[:, groups : groups + experts]
    home_part = jnp.concatenate(
        [products[:, :groups]]
        + [
            jnp.sum(jnp.where(expert_iota == routing[:, k : k + 1], expert_part, 0.0), 1, keepdims=True)
            for k in range(top)
        ]
        + [products[:, groups + experts :], jnp.sum(residual_own * residual_own, 1, keepdims=True)],
        1,
    )
    home_count = home_part.shape[1]

    gain_ffn = norm_gain_ffn.astype(jnp.float32)
    gain_own = lax.dynamic_slice_in_dim(gain_ffn, offset, feat, 0)
    units = dense_gate.shape[1]
    share = total // n_tp
    scaled = (rows * gain_own).astype(jnp.bfloat16)
    dense_terms = jnp.dot(
        scaled, jnp.concatenate([dense_gate, dense_up], 1), preferred_element_type=jnp.float32
    ).astype(jnp.bfloat16)
    squares_high, squares_low = to_pair(jnp.sum(rows * rows, 1).reshape(n_tp, 1, share))
    home_high, home_low = to_pair(home_part.reshape(1, seq_count * home_count))
    lanes = 2 * units
    half = n_ep * cap // 2

    def lane_pad(array):
        return jnp.pad(array, [(0, 0)] * (array.ndim - 1) + [(0, lanes - array.shape[-1])])

    common = jnp.concatenate(
        [
            jnp.concatenate([picked[:half], picked[half:]], 1),
            lane_pad(home_high),
            lane_pad(home_low),
        ],
        0,
    )
    gathered = exchange(
        jnp.concatenate(
            [
                dense_terms.reshape(n_tp, share, lanes),
                jnp.broadcast_to(common[None], (n_tp, *common.shape)),
                lane_pad(squares_high),
                lane_pad(squares_low),
            ],
            1,
        ),
        "tp",
    )
    at_home = share + half
    at_squares = at_home + 2
    dense_both = sum_lead(gathered[:, :share])
    home_sum = jnp.sum(
        gathered[:, at_home:at_squares, : seq_count * home_count].astype(jnp.float32), (0, 1)
    ).reshape(seq_count, home_count)
    squares = jnp.sum(gathered[:, at_squares:, :share].astype(jnp.float32), (0, 1))
    scale = lax.rsqrt(squares / width + epsilon)[:, None]
    dense_act = (
        jax.nn.silu(dense_both[:, :units] * scale) * (dense_both[:, units:] * scale)
    ).astype(jnp.bfloat16)

    whole = (
        gathered[:, share:at_home]
        .reshape(n_tp, half, 2, feat)
        .transpose(2, 1, 0, 3)
        .reshape(2 * half, width)
        .astype(jnp.float32)
    )
    inverse_rows = lax.rsqrt(jnp.mean(whole * whole, -1, keepdims=True) + epsilon)
    hidden_in = (whole * inverse_rows * gain_ffn).astype(jnp.bfloat16)
    gate_acc = jnp.dot(hidden_in, expert_gate[0], preferred_element_type=jnp.float32)
    up_acc = jnp.dot(hidden_in, expert_up[0], preferred_element_type=jnp.float32)
    hidden = (jax.nn.silu(gate_acc) * up_acc).astype(jnp.bfloat16)
    expert_terms = jnp.dot(hidden, expert_down[0], preferred_element_type=jnp.float32)
    expert_terms = jnp.moveaxis(
        expert_terms.astype(jnp.bfloat16).reshape(2 * half, n_tp, feat), 1, 0
    )

    reached = 2 * half + share
    summed = exchange(
        jnp.concatenate(
            [
                expert_terms,
                jnp.broadcast_to(dense_act[None], (n_tp, share, units)),
                jnp.zeros((n_tp, round_up(reached) - reached, feat), jnp.bfloat16),
            ],
            1,
        ),
        "tp",
    )
    expert_out = sum_lead(summed[:, : 2 * half]).astype(jnp.bfloat16)
    acts = summed[:, 2 * half : reached].reshape(total, units)
    dense_term = jnp.dot(acts, dense_down, preferred_element_type=jnp.float32)

    returned = exchange(
        jnp.concatenate(
            [
                dense_term.astype(jnp.bfloat16).reshape(n_ep, seq_count, feat),
                expert_out.reshape(n_ep, cap, feat),
                jnp.zeros((n_ep, both_pad - both, feat), jnp.bfloat16),
            ],
            1,
        ),
        "ep",
    )
    dense = sum_lead(returned[:, :seq_count])
    flat_back = returned[:, seq_count:both].reshape(experts * cap, feat)

    inverse_two = lax.rsqrt(home_sum[:, home_count - 1 :] / width + epsilon)
    logits = home_sum[:, : home_count - 1] * inverse_two
    group_exp = jnp.exp(logits[:, :groups])
    group_iota = lax.broadcasted_iota(jnp.int32, (1, groups), 1)
    own_group = jnp.sum(
        jnp.where(group_iota == routing[:, :1] // per_group, group_exp, 0.0), 1, keepdims=True
    )
    group_prob = own_group / jnp.sum(group_exp, 1, keepdims=True)
    chosen_exp = jnp.exp(logits[:, groups : groups + top])
    route_gate = group_prob * chosen_exp / jnp.sum(chosen_exp, 1, keepdims=True)
    row_iota = lax.broadcasted_iota(jnp.int32, (1, experts * cap), 1)
    moe = jnp.zeros((seq_count, feat), jnp.float32)
    for which in range(top):
        select = (index[:, which : which + 1] == row_iota).astype(jnp.bfloat16)
        moe = moe + route_gate[:, which : which + 1] * jnp.dot(
            select, flat_back, preferred_element_type=jnp.float32
        )
    branch = jax.nn.sigmoid(logits[:, groups + top :])
    mixed = (residual_own + moe + branch * dense).astype(jnp.bfloat16)
    return (mixed, fresh_keys, fresh_values)


def solution(mesh):
    placed = (
        P("ep", None),
        P(),
        P("tp", None),
        P("tp", None),
        P("tp", None),
        P("tp"),
        P("ep", "tp", None),
        P("ep", "tp", None),
        P("ep"),
        P("tp", None),
        P(),
        P(),
        P(),
        P("ep", None),
        P("ep", None, "tp"),
        P("ep", None, "tp"),
        P("ep", "tp", None),
        P(),
        P("tp", "ep"),
        P("tp", "ep"),
        P("ep", "tp"),
    )
    return jax.shard_map(
        local,
        mesh=mesh,
        in_specs=placed,
        out_specs=(P("ep", "tp"), P("ep", "tp"), P("ep", "tp")),
        check_vma=False,
    )
```

```python
import jax
import jax.numpy as jnp
from jax import lax
from jax.sharding import PartitionSpec as P


epsilon = 1e-06


def project_rows(normed, weight):
    return lax.dot_general(
        normed, weight, (((1,), (1,)), ((), ())), preferred_element_type=jnp.float32
    )


def stick_weights(scores, inside):
    positions = scores.shape[1]
    log_keep = jnp.where(inside, jax.nn.log_sigmoid(-scores), 0.0)
    rows = lax.broadcasted_iota(jnp.int32, (positions, positions), 0)
    columns = lax.broadcasted_iota(jnp.int32, (positions, positions), 1)
    after = (rows > columns).astype(jnp.float32)
    remain = jnp.dot(
        log_keep, after, precision=lax.Precision.HIGHEST, preferred_element_type=jnp.float32
    )
    return jnp.where(inside, jnp.exp(jax.nn.log_sigmoid(scores) + remain), 0.0)


def exchange(array, axis):
    return lax.all_to_all(array, axis, 0, 0, tiled=True)


def to_pair(value):
    high = lax.reduce_precision(value, 8, 7)
    return high.astype(jnp.bfloat16), (value - high).astype(jnp.bfloat16)


def round_up(count, unit=8):
    return -(-count // unit) * unit


def sum_lead(array):
    return jnp.sum(array.astype(jnp.float32), axis=0)


def local(
    stream,
    norm_gain_mix,
    query_weight,
    key_weight,
    value_weight,
    score_offset,
    cache_keys,
    cache_values,
    lengths,
    out_weight,
    norm_gain_ffn,
    group_weight,
    router_weight,
    routing,
    expert_gate,
    expert_up,
    expert_down,
    branch_gate,
    dense_gate,
    dense_up,
    dense_down,
):
    seq_count = stream.shape[0]
    width = stream.shape[1]
    n_tp = lax.axis_size("tp")
    n_ep = lax.axis_size("ep")
    tp_rank = lax.axis_index("tp")
    feat = width // n_tp
    offset = tp_rank * feat
    rows_pad = round_up(seq_count)

    stream_f = stream.astype(jnp.float32)
    inverse = lax.rsqrt(jnp.mean(stream_f * stream_f, -1, keepdims=True) + epsilon)
    normed = (stream_f * inverse * norm_gain_mix.astype(jnp.float32)).astype(jnp.bfloat16)
    queries = project_rows(normed, query_weight).astype(jnp.bfloat16)
    fresh_keys = project_rows(normed, key_weight).astype(jnp.bfloat16)
    fresh_values = project_rows(normed, value_weight).astype(jnp.bfloat16)
    head_size = queries.shape[1]
    cache_len = cache_keys.shape[2]
    scores = jnp.einsum("sd,sdl->sl", queries, cache_keys, preferred_element_type=jnp.float32)
    scores = scores * head_size ** (-0.5) + score_offset[0]
    inside = lax.broadcasted_iota(jnp.int32, (1, cache_len), 1) < lengths[:, None]
    weights = stick_weights(scores, inside).astype(jnp.bfloat16)
    heads_out = jnp.einsum("sl,sdl->sd", weights, cache_values, preferred_element_type=jnp.float32)
    heads_out = jnp.pad(heads_out.astype(jnp.bfloat16), ((0, rows_pad - seq_count), (0, 0)))
    partial_value = jnp.dot(heads_out, out_weight, preferred_element_type=jnp.float32)
    terms = partial_value.astype(jnp.bfloat16).reshape(rows_pad, n_tp, feat)
    attn = sum_lead(exchange(jnp.moveaxis(terms, 1, 0), "tp"))[:seq_count]

    residual = (
        lax.dynamic_slice_in_dim(stream, offset, feat, 1).astype(jnp.float32)
        + attn.astype(jnp.bfloat16).astype(jnp.float32)
    ).astype(jnp.bfloat16)
    residual_own = residual.astype(jnp.float32)

    experts = router_weight.shape[1]
    groups = group_weight.shape[1]
    per_group = experts // groups
    top = routing.shape[1]
    cap = 2 * ((seq_count + experts - 1) // experts)
    expert_iota = lax.broadcasted_iota(jnp.int32, (1, experts), 1)
    pair_expert = routing.reshape(seq_count * top)
    onehot = (pair_expert[:, None] == expert_iota).astype(jnp.int32)
    before = jnp.cumsum(onehot, 0) - onehot
    slot = jnp.sum(before * onehot, 1)
    index = (pair_expert * cap + slot).reshape(seq_count, top)
    slot_iota = lax.broadcasted_iota(jnp.int32, (experts * cap, 1, 1), 0)
    dispatch = jnp.sum((index[None, :, :] == slot_iota).astype(jnp.int32), 2).astype(jnp.bfloat16)
    send = jnp.dot(dispatch, residual, preferred_element_type=jnp.float32).astype(jnp.bfloat16)

    both = seq_count + cap
    both_pad = round_up(both)
    arrived = exchange(
        jnp.concatenate(
            [
                jnp.broadcast_to(residual[None], (n_ep, seq_count, feat)),
                send.reshape(n_ep, cap, feat),
                jnp.zeros((n_ep, both_pad - both, feat), jnp.bfloat16),
            ],
            1,
        ),
        "ep",
    )
    total = n_ep * seq_count
    rows = arrived[:, :seq_count].reshape(total, feat).astype(jnp.float32)
    picked = arrived[:, seq_count:both].reshape(n_ep * cap, feat)

    home_weights = jnp.concatenate(
        [
            lax.dynamic_slice_in_dim(group_weight, offset, feat, 0),
            lax.dynamic_slice_in_dim(router_weight, offset, feat, 0),
            lax.dynamic_slice_in_dim(branch_gate, offset, feat, 0)[:, None],
        ],
        1,
    )
    products = jnp.dot(residual, home_weights, preferred_element_type=jnp.float32)
    expert_part = products[:, groups : groups + experts]
    home_part = jnp.concatenate(
        [products[:, :groups]]
        + [
            jnp.sum(jnp.where(expert_iota == routing[:, k : k + 1], expert_part, 0.0), 1, keepdims=True)
            for k in range(top)
        ]
        + [products[:, groups + experts :], jnp.sum(residual_own * residual_own, 1, keepdims=True)],
        1,
    )
    home_count = home_part.shape[1]

    gain_ffn = norm_gain_ffn.astype(jnp.float32)
    gain_own = lax.dynamic_slice_in_dim(gain_ffn, offset, feat, 0)
    units = dense_gate.shape[1]
    share = total // n_tp
    scaled = (rows * gain_own).astype(jnp.bfloat16)
    dense_terms = jnp.dot(
        scaled, jnp.concatenate([dense_gate, dense_up], 1), preferred_element_type=jnp.float32
    ).astype(jnp.bfloat16)
    squares_high, squares_low = to_pair(jnp.sum(rows * rows, 1).reshape(n_tp, 1, share))
    home_high, home_low = to_pair(home_part.reshape(1, seq_count * home_count))
    lanes = 2 * units

    def lane_pad(array):
        return jnp.pad(array, [(0, 0)] * (array.ndim - 1) + [(0, lanes - array.shape[-1])])

    leaving = jnp.concatenate(
        [
            dense_terms.reshape(n_tp, share, lanes),
            lane_pad(squares_high),
            lane_pad(squares_low),
            jnp.broadcast_to(lane_pad(home_high)[None], (n_tp, 1, lanes)),
            jnp.broadcast_to(lane_pad(home_low)[None], (n_tp, 1, lanes)),
        ],
        1,
    )
    gathered = exchange(leaving, "tp")
    whole = lax.all_gather(picked, "tp", axis=1, tiled=True)
    whole = whole.astype(jnp.float32)
    at_home = share + 2
    dense_both = sum_lead(gathered[:, :share])
    home_sum = jnp.sum(
        gathered[:, at_home:, : seq_count * home_count].astype(jnp.float32), (0, 1)
    ).reshape(seq_count, home_count)
    squares = jnp.sum(gathered[:, share:at_home, :share].astype(jnp.float32), (0, 1))
    scale = lax.rsqrt(squares / width + epsilon)[:, None]
    dense_act = (
        jax.nn.silu(dense_both[:, :units] * scale) * (dense_both[:, units:] * scale)
    ).astype(jnp.bfloat16)

    inverse_rows = lax.rsqrt(jnp.mean(whole * whole, -1, keepdims=True) + epsilon)
    hidden_in = (whole * inverse_rows * gain_ffn).astype(jnp.bfloat16)
    gate_acc = jnp.dot(hidden_in, expert_gate[0], preferred_element_type=jnp.float32)
    up_acc = jnp.dot(hidden_in, expert_up[0], preferred_element_type=jnp.float32)
    hidden = (jax.nn.silu(gate_acc) * up_acc).astype(jnp.bfloat16)
    expert_terms = jnp.dot(hidden, expert_down[0], preferred_element_type=jnp.float32)
    expert_terms = jnp.moveaxis(
        expert_terms.astype(jnp.bfloat16).reshape(n_ep * cap, n_tp, feat), 1, 0
    )

    summed = exchange(expert_terms, "tp")
    acts = lax.all_gather(dense_act, "tp", axis=0, tiled=True)
    expert_out = sum_lead(summed).astype(jnp.bfloat16)
    dense_term = jnp.dot(acts, dense_down, preferred_element_type=jnp.float32)

    returned = exchange(
        jnp.concatenate(
            [
                dense_term.astype(jnp.bfloat16).reshape(n_ep, seq_count, feat),
                expert_out.reshape(n_ep, cap, feat),
                jnp.zeros((n_ep, both_pad - both, feat), jnp.bfloat16),
            ],
            1,
        ),
        "ep",
    )
    dense = sum_lead(returned[:, :seq_count])
    flat_back = returned[:, seq_count:both].reshape(experts * cap, feat)

    inverse_two = lax.rsqrt(home_sum[:, home_count - 1 :] / width + epsilon)
    logits = home_sum[:, : home_count - 1] * inverse_two
    group_exp = jnp.exp(logits[:, :groups])
    group_iota = lax.broadcasted_iota(jnp.int32, (1, groups), 1)
    own_group = jnp.sum(
        jnp.where(group_iota == routing[:, :1] // per_group, group_exp, 0.0), 1, keepdims=True
    )
    group_prob = own_group / jnp.sum(group_exp, 1, keepdims=True)
    chosen_exp = jnp.exp(logits[:, groups : groups + top])
    route_gate = group_prob * chosen_exp / jnp.sum(chosen_exp, 1, keepdims=True)
    row_iota = lax.broadcasted_iota(jnp.int32, (1, experts * cap), 1)
    moe = jnp.zeros((seq_count, feat), jnp.float32)
    for which in range(top):
        select = (index[:, which : which + 1] == row_iota).astype(jnp.bfloat16)
        moe = moe + route_gate[:, which : which + 1] * jnp.dot(
            select, flat_back, preferred_element_type=jnp.float32
        )
    branch = jax.nn.sigmoid(logits[:, groups + top :])
    mixed = (residual_own + moe + branch * dense).astype(jnp.bfloat16)
    return (mixed, fresh_keys, fresh_values)


def solution(mesh):
    placed = (
        P("ep", None),
        P(),
        P("tp", None),
        P("tp", None),
        P("tp", None),
        P("tp"),
        P("ep", "tp", None),
        P("ep", "tp", None),
        P("ep"),
        P("tp", None),
        P(),
        P(),
        P(),
        P("ep", None),
        P("ep", None, "tp"),
        P("ep", None, "tp"),
        P("ep", "tp", None),
        P(),
        P("tp", "ep"),
        P("tp", "ep"),
        P("ep", "tp"),
    )
    return jax.shard_map(
        local,
        mesh=mesh,
        in_specs=placed,
        out_specs=(P("ep", "tp"), P("ep", "tp"), P("ep", "tp")),
        check_vma=False,
    )
```

```python
import jax
import jax.numpy as jnp
from jax import lax
from jax.sharding import Mesh, PartitionSpec as P

epsilon = 1e-06
TP = ("y", "core")


def project_rows(normed, weight):
    return lax.dot_general(
        normed, weight, (((1,), (1,)), ((), ())), preferred_element_type=jnp.float32
    )


def stick_weights(scores, inside):
    positions = scores.shape[1]
    log_keep = jnp.where(inside, jax.nn.log_sigmoid(-scores), 0.0)
    rows = lax.broadcasted_iota(jnp.int32, (positions, positions), 0)
    columns = lax.broadcasted_iota(jnp.int32, (positions, positions), 1)
    after = (rows > columns).astype(jnp.float32)
    remain = jnp.dot(
        log_keep, after, precision=lax.Precision.HIGHEST, preferred_element_type=jnp.float32
    )
    return jnp.where(inside, jnp.exp(jax.nn.log_sigmoid(scores) + remain), 0.0)


def exchange(array, axis):
    return lax.all_to_all(array, axis, 0, 0, tiled=True)


def to_pair(value):
    high = lax.reduce_precision(value, 8, 7)
    return high.astype(jnp.bfloat16), (value - high).astype(jnp.bfloat16)


def round_up(count, unit=8):
    return -(-count // unit) * unit


def sum_lead(array):
    return jnp.sum(array.astype(jnp.float32), axis=0)


def local(
    stream,
    norm_gain_mix,
    query_weight,
    key_weight,
    value_weight,
    score_offset,
    cache_keys,
    cache_values,
    lengths,
    out_weight,
    norm_gain_ffn,
    group_weight,
    router_weight,
    routing,
    expert_gate,
    expert_up,
    expert_down,
    branch_gate,
    dense_gate,
    dense_up,
    dense_down,
):
    seq_count = stream.shape[0]
    width = stream.shape[1]
    n_tp = lax.axis_size(TP)
    n_ep = lax.axis_size("ep")
    n_y = lax.axis_size("y")
    n_core = lax.axis_size("core")
    core = lax.axis_index("core")
    feat = width // n_tp
    offset = lax.axis_index(TP) * feat
    wide = n_core * feat
    wide_offset = lax.axis_index("y") * wide

    swap = [(0, 1), (1, 0)]
    with jax.named_scope("swap_gate"):
        other_gate = lax.ppermute(expert_gate[0], "core", swap)
    with jax.named_scope("swap_up"):
        other_up = lax.ppermute(expert_up[0], "core", swap)
    with jax.named_scope("swap_down"):
        other_down = lax.ppermute(expert_down[0], "core", swap)
    with jax.named_scope("dense_gather"):
        dense_pair = lax.all_gather(
            jnp.concatenate([dense_gate, dense_up, dense_down], 1), "core"
        )
    units = dense_gate.shape[1]
    dense_in = dense_pair[:, :, : 2 * units]
    dense_out = dense_pair[:, :, 2 * units :]
    rows_pad = round_up(seq_count)

    stream_f = stream.astype(jnp.float32)
    inverse = lax.rsqrt(jnp.mean(stream_f * stream_f, -1, keepdims=True) + epsilon)
    normed = (stream_f * inverse * norm_gain_mix.astype(jnp.float32)).astype(jnp.bfloat16)
    queries = project_rows(normed, query_weight).astype(jnp.bfloat16)
    fresh_keys = project_rows(normed, key_weight).astype(jnp.bfloat16)
    fresh_values = project_rows(normed, value_weight).astype(jnp.bfloat16)
    head_size = queries.shape[1]
    cache_len = cache_keys.shape[2]
    scores = jnp.einsum("sd,sdl->sl", queries, cache_keys, preferred_element_type=jnp.float32)
    scores = scores * head_size ** (-0.5) + score_offset[0]
    inside = lax.broadcasted_iota(jnp.int32, (1, cache_len), 1) < lengths[:, None]
    weights = stick_weights(scores, inside).astype(jnp.bfloat16)
    heads_out = jnp.einsum("sl,sdl->sd", weights, cache_values, preferred_element_type=jnp.float32)
    heads_out = jnp.pad(heads_out.astype(jnp.bfloat16), ((0, rows_pad - seq_count), (0, 0)))
    partial_value = jnp.dot(heads_out, out_weight, preferred_element_type=jnp.float32)
    terms = partial_value.astype(jnp.bfloat16).reshape(rows_pad, n_tp, feat)
    attn = sum_lead(exchange(jnp.moveaxis(terms, 1, 0), TP))[:seq_count]

    residual = (
        lax.dynamic_slice_in_dim(stream, offset, feat, 1).astype(jnp.float32)
        + attn.astype(jnp.bfloat16).astype(jnp.float32)
    ).astype(jnp.bfloat16)
    residual_own = residual.astype(jnp.float32)
    pair = lax.all_gather(residual, "core", axis=1, tiled=True)

    experts = router_weight.shape[1]
    groups = group_weight.shape[1]
    per_group = experts // groups
    top = routing.shape[1]
    cap = 2 * ((seq_count + experts - 1) // experts)
    expert_iota = lax.broadcasted_iota(jnp.int32, (1, experts), 1)
    pair_expert = routing.reshape(seq_count * top)
    onehot = (pair_expert[:, None] == expert_iota).astype(jnp.int32)
    before = jnp.cumsum(onehot, 0) - onehot
    slot = jnp.sum(before * onehot, 1)
    index = (pair_expert * cap + slot).reshape(seq_count, top)
    slot_iota = n_core * lax.broadcasted_iota(jnp.int32, (experts, 1, 1), 0) + core
    dispatch = jnp.sum((index[None, :, :] == slot_iota).astype(jnp.int32), 2).astype(jnp.bfloat16)
    send = jnp.dot(dispatch, pair, preferred_element_type=jnp.float32).astype(jnp.bfloat16)

    part = seq_count // n_core
    own_rows = lax.dynamic_slice_in_dim(pair, core * part, part, 0)
    both = seq_count + n_core
    both_pad = round_up(both)
    arrived = exchange(
        jnp.concatenate(
            [
                jnp.broadcast_to(own_rows[None, :, :feat], (n_ep, part, feat)),
                jnp.broadcast_to(own_rows[None, :, feat:], (n_ep, part, feat)),
                send.reshape(n_ep, n_core, feat),
                jnp.zeros((n_ep, both_pad - both, feat), jnp.bfloat16),
            ],
            1,
        ),
        "ep",
    )
    total = n_ep * part
    rows = [
        arrived[:, :part].reshape(total, feat).astype(jnp.float32),
        arrived[:, part:seq_count].reshape(total, feat).astype(jnp.float32),
    ]
    picked = arrived[:, seq_count:both].reshape(n_ep, wide)

    home_weights = jnp.concatenate(
        [
            lax.dynamic_slice_in_dim(group_weight, wide_offset, wide, 0),
            lax.dynamic_slice_in_dim(router_weight, wide_offset, wide, 0),
            lax.dynamic_slice_in_dim(branch_gate, wide_offset, wide, 0)[:, None],
        ],
        1,
    )
    products = jnp.dot(pair, home_weights, preferred_element_type=jnp.float32)
    expert_part = products[:, groups : groups + experts]
    home_part = jnp.concatenate(
        [products[:, :groups]]
        + [
            jnp.sum(jnp.where(expert_iota == routing[:, k : k + 1], expert_part, 0.0), 1, keepdims=True)
            for k in range(top)
        ]
        + [products[:, groups + experts :], jnp.sum(jnp.square(pair.astype(jnp.float32)), 1, keepdims=True)],
        1,
    )
    home_count = home_part.shape[1]

    gain_ffn = norm_gain_ffn.astype(jnp.float32)
    gain_wide = lax.dynamic_slice_in_dim(gain_ffn, wide_offset, wide, 0)
    share = total // n_y
    dense_terms = jnp.zeros((total, 2 * units), jnp.float32)
    for k in range(n_core):
        scaled = (rows[k] * gain_wide[k * feat : (k + 1) * feat]).astype(jnp.bfloat16)
        dense_terms += jnp.dot(scaled, dense_in[k], preferred_element_type=jnp.float32)
    dense_terms = dense_terms.astype(jnp.bfloat16)
    squares_part = sum(jnp.sum(r * r, 1) for r in rows)
    squares_high, squares_low = to_pair(squares_part.reshape(n_y, 1, share))
    home_high, home_low = to_pair(home_part.reshape(1, seq_count * home_count))
    lanes = 2 * units

    def lane_pad(array):
        return jnp.pad(array, [(0, 0)] * (array.ndim - 1) + [(0, lanes - array.shape[-1])])

    common = jnp.concatenate(
        [
            picked,
            lane_pad(home_high),
            lane_pad(home_low),
        ],
        0,
    )
    gathered = exchange(
        jnp.concatenate(
            [
                dense_terms.reshape(n_y, share, lanes),
                jnp.broadcast_to(common[None], (n_y, *common.shape)),
                lane_pad(squares_high),
                lane_pad(squares_low),
            ],
            1,
        ),
        "y",
    )
    at_home = share + n_ep
    at_squares = at_home + 2
    dense_both = sum_lead(gathered[:, :share])
    home_sum = jnp.sum(
        gathered[:, at_home:at_squares, : seq_count * home_count].astype(jnp.float32), (0, 1)
    ).reshape(seq_count, home_count)
    squares = jnp.sum(gathered[:, at_squares:, :share].astype(jnp.float32), (0, 1))
    scale = lax.rsqrt(squares / width + epsilon)[:, None]
    dense_act = (
        jax.nn.silu(dense_both[:, :units] * scale) * (dense_both[:, units:] * scale)
    ).astype(jnp.bfloat16)

    whole = (
        jnp.moveaxis(gathered[:, share:at_home], 0, 1).reshape(n_ep, width).astype(jnp.float32)
    )
    inverse_rows = lax.rsqrt(jnp.mean(whole * whole, -1, keepdims=True) + epsilon)
    hidden_in = (whole * inverse_rows * gain_ffn).astype(jnp.bfloat16)
    expert_terms = jnp.zeros((n_ep, width), jnp.float32)
    for gate_w, up_w, down_w in (
        (expert_gate[0], expert_up[0], expert_down[0]),
        (other_gate, other_up, other_down),
    ):
        gate_acc = jnp.dot(hidden_in, gate_w, preferred_element_type=jnp.float32)
        up_acc = jnp.dot(hidden_in, up_w, preferred_element_type=jnp.float32)
        hidden = (jax.nn.silu(gate_acc) * up_acc).astype(jnp.bfloat16)
        expert_terms += jnp.dot(hidden, down_w, preferred_element_type=jnp.float32)
    expert_terms = jnp.moveaxis(
        expert_terms.astype(jnp.bfloat16).reshape(n_ep, n_tp, feat), 1, 0
    ).reshape(n_y, n_core * n_ep, feat)

    at_act = n_core * n_ep
    reached = at_act + share
    summed = exchange(
        jnp.concatenate(
            [
                expert_terms,
                jnp.broadcast_to(dense_act[None], (n_y, share, units)),
                jnp.zeros((n_y, round_up(reached) - reached, feat), jnp.bfloat16),
            ],
            1,
        ),
        "y",
    )
    expert_out = sum_lead(summed[:, :at_act]).astype(jnp.bfloat16)
    acts = summed[:, at_act:reached].reshape(total, units)
    dense_terms_out = [
        jnp.dot(acts, dense_out[k], preferred_element_type=jnp.float32)
        .astype(jnp.bfloat16)
        .reshape(n_ep, part, feat)
        for k in range(n_core)
    ]

    returned = exchange(
        jnp.concatenate(
            dense_terms_out
            + [
                jnp.moveaxis(expert_out.reshape(n_core, n_ep, feat), 0, 1),
                jnp.zeros((n_ep, both_pad - both, feat), jnp.bfloat16),
            ],
            1,
        ),
        "ep",
    )
    dense = sum_lead(returned[:, :seq_count])
    dense = jnp.concatenate([dense[:part], dense[part:]], 1)
    back = returned[:, seq_count:both].reshape(n_ep, wide)

    inverse_two = lax.rsqrt(home_sum[:, home_count - 1 :] / width + epsilon)
    logits = home_sum[:, : home_count - 1] * inverse_two
    group_exp = jnp.exp(logits[:, :groups])
    group_iota = lax.broadcasted_iota(jnp.int32, (1, groups), 1)
    own_group = jnp.sum(
        jnp.where(group_iota == routing[:, :1] // per_group, group_exp, 0.0), 1, keepdims=True
    )
    group_prob = own_group / jnp.sum(group_exp, 1, keepdims=True)
    chosen_exp = jnp.exp(logits[:, groups : groups + top])
    route_gate = group_prob * chosen_exp / jnp.sum(chosen_exp, 1, keepdims=True)
    row_iota = n_core * lax.broadcasted_iota(jnp.int32, (1, experts), 1) + core
    mixture = jnp.zeros((seq_count, wide), jnp.float32)
    for which in range(top):
        select = (index[:, which : which + 1] == row_iota).astype(jnp.bfloat16)
        mixture = mixture + route_gate[:, which : which + 1] * jnp.dot(
            select, back, preferred_element_type=jnp.float32
        )
    branch = jax.nn.sigmoid(logits[:, groups + top :])
    mine = lax.broadcasted_iota(jnp.int32, (seq_count, 1), 0) // part == core
    mixture = mixture + branch * jnp.where(mine, jnp.concatenate([dense] * n_core, 0), 0.0)
    mixture = jnp.sum(lax.all_gather(mixture, "core"), 0)
    mixed = (residual_own + lax.dynamic_slice_in_dim(mixture, core * feat, feat, 1)).astype(
        jnp.bfloat16
    )
    return (mixed, fresh_keys, fresh_values)


def solution(mesh):
    n_ep, n_tp = mesh.devices.shape
    split = Mesh(mesh.devices.reshape(n_ep, n_tp // 2, 2), ("ep", "y", "core"))
    placed = (
        P("ep", None),
        P(),
        P(TP, None),
        P(TP, None),
        P(TP, None),
        P(TP),
        P("ep", TP, None),
        P("ep", TP, None),
        P("ep"),
        P(TP, None),
        P(),
        P(),
        P(),
        P("ep", None),
        P("ep", None, TP),
        P("ep", None, TP),
        P("ep", TP, None),
        P(),
        P(TP, "ep"),
        P(TP, "ep"),
        P("ep", TP),
    )
    return jax.shard_map(
        local,
        mesh=split,
        in_specs=placed,
        out_specs=(P("ep", TP), P("ep", TP), P("ep", TP)),
        check_vma=False,
    )
```

```python
import jax
import jax.numpy as jnp
from jax import lax
from jax.experimental import pallas as pl
from jax.experimental.pallas import tpu as pltpu
from jax.sharding import Mesh, PartitionSpec as P

epsilon = 1e-06
TP = ("y", "core")


def across(left, right):
    return lax.dot_general(
        left, right, (((1,), (1,)), ((), ())), preferred_element_type=jnp.float32
    )


def attend_kernel(
    offset_ref,
    lengths_ref,
    stream_ref,
    gain_ref,
    query_ref,
    key_ref,
    value_ref,
    keys_ref,
    values_ref,
    out_weight_ref,
    terms_ref,
    fresh_keys_ref,
    fresh_values_ref,
):
    count, width = stream_ref.shape
    head_size, cache_len = keys_ref.shape[1:]
    n_blocks, rows, feat = terms_ref.shape
    stream_f = stream_ref[...].astype(jnp.float32)
    inverse = lax.rsqrt(jnp.mean(stream_f * stream_f, -1, keepdims=True) + epsilon)
    normed = (stream_f * inverse * gain_ref[...].astype(jnp.float32)[None]).astype(jnp.bfloat16)
    queries = across(normed, query_ref[...])
    queries = jnp.concatenate([queries, jnp.zeros((rows - count, head_size), jnp.float32)], 0)
    queries = queries.astype(jnp.bfloat16)
    row = lax.broadcasted_iota(jnp.int32, (rows, 1), 0)
    scores = jnp.zeros((rows, cache_len), jnp.float32)
    for s in range(count):
        each = jnp.dot(queries, keys_ref[s], preferred_element_type=jnp.float32)
        scores = jnp.where(row == s, each, scores)
    scores = scores * head_size ** (-0.5) + offset_ref[0]
    filled = jnp.zeros((rows, 1), jnp.int32)
    for s in range(count):
        filled = jnp.where(row == s, lengths_ref[s], filled)
    inside = lax.broadcasted_iota(jnp.int32, (rows, cache_len), 1) < filled
    tail = jnp.log1p(jnp.exp(-jnp.abs(scores)))
    log_keep = jnp.where(inside, jnp.minimum(-scores, 0.0) - tail, 0.0)
    after = (
        lax.broadcasted_iota(jnp.int32, (cache_len, cache_len), 0)
        > lax.broadcasted_iota(jnp.int32, (cache_len, cache_len), 1)
    ).astype(jnp.float32)
    remain = jnp.dot(
        log_keep, after, precision=lax.Precision.HIGHEST, preferred_element_type=jnp.float32
    )
    weights = jnp.where(inside, jnp.exp(jnp.minimum(scores, 0.0) - tail + remain), 0.0)
    weights = weights.astype(jnp.bfloat16)
    heads_out = jnp.zeros((rows, head_size), jnp.float32)
    for s in range(count):
        heads_out = jnp.where(row == s, across(weights, values_ref[s]), heads_out)
    terms = jnp.dot(
        heads_out.astype(jnp.bfloat16), out_weight_ref[...], preferred_element_type=jnp.float32
    ).astype(jnp.bfloat16)
    for k in range(n_blocks):
        terms_ref[k] = terms[:, k * feat : (k + 1) * feat]
    fresh_keys_ref[...] = across(normed, key_ref[...]).astype(jnp.bfloat16)
    fresh_values_ref[...] = across(normed, value_ref[...]).astype(jnp.bfloat16)


def attend(
    stream, gain, query_w, key_w, value_w, offset, keys, values, lengths, out_weight, n_tp, rows
):
    count, width = stream.shape
    whole = pl.BlockSpec(memory_space=pltpu.VMEM)
    fresh = jax.ShapeDtypeStruct((count, key_w.shape[0]), jnp.bfloat16)
    return pl.pallas_call(
        attend_kernel,
        out_shape=(
            jax.ShapeDtypeStruct((n_tp, rows, width // n_tp), jnp.bfloat16),
            fresh,
            fresh,
        ),
        in_specs=[pl.BlockSpec(memory_space=pltpu.SMEM)] * 2 + [whole] * 8,
        out_specs=(whole, whole, whole),
        name="attend",
    )(offset, lengths, stream, gain, query_w, key_w, value_w, keys, values, out_weight)


def silu(value):
    return value * jax.nn.sigmoid(value)


def expert_kernel(
    gathered_ref,
    gain_ref,
    gate_hbm,
    up_hbm,
    down_hbm,
    other_gate_hbm,
    other_up_hbm,
    other_down_hbm,
    out_ref,
    home_ref,
    hidden_ref,
    gate_ref,
    up_ref,
    down_ref,
    other_gate_ref,
    other_up_ref,
    other_down_ref,
    sems,
):
    copies = [
        pltpu.make_async_copy(source, target, sems.at[k])
        for k, (source, target) in enumerate(
            (
                (gate_hbm, gate_ref),
                (up_hbm, up_ref),
                (other_gate_hbm, other_gate_ref),
                (other_up_hbm, other_up_ref),
                (down_hbm, down_ref),
                (other_down_hbm, other_down_ref),
            )
        )
    ]
    for copy in copies:
        copy.start()
    n_y, rows_in, lanes = gathered_ref.shape
    n_rows, width = hidden_ref.shape
    feat = out_ref.shape[2]
    units = lanes // 2
    at_expert = rows_in - n_rows
    share = at_expert - 4

    both = gathered_ref[0, :at_expert].astype(jnp.float32)
    for k in range(1, n_y):
        both = both + gathered_ref[k, :at_expert].astype(jnp.float32)
    home_ref[...] = both[share:]
    squares = both[share + 2 : share + 3] + both[share + 3 : share + 4]
    diagonal = lax.broadcasted_iota(jnp.int32, (at_expert, lanes), 0) == lax.broadcasted_iota(
        jnp.int32, (at_expert, lanes), 1
    )
    column = jnp.sum(jnp.where(diagonal, squares, 0.0), 1, keepdims=True)
    both = both * lax.rsqrt(column / width + epsilon)
    act = (silu(both[:, :units]) * both[:, units:]).astype(jnp.bfloat16)
    for k in range(n_y):
        out_ref[k, 2 * n_rows :] = act

    squares = jnp.zeros((n_rows, 1), jnp.float32)
    for k in range(n_y):
        rows = gathered_ref[k, at_expert:].astype(jnp.float32)
        squares = squares + jnp.sum(rows * rows, 1, keepdims=True)
    inverse = lax.rsqrt(squares / width + epsilon)
    for k in range(n_y):
        rows = gathered_ref[k, at_expert:].astype(jnp.float32)
        gain = gain_ref[pl.ds(k * lanes, lanes)].astype(jnp.float32)[None]
        hidden_ref[:, k * lanes : (k + 1) * lanes] = (rows * inverse * gain).astype(jnp.bfloat16)
    hidden_in = hidden_ref[...]
    acts = []
    for k, (gate_w, up_w) in enumerate(((gate_ref, up_ref), (other_gate_ref, other_up_ref))):
        copies[2 * k].wait()
        gate = jnp.dot(hidden_in, gate_w[...], preferred_element_type=jnp.float32)
        copies[2 * k + 1].wait()
        up = jnp.dot(hidden_in, up_w[...], preferred_element_type=jnp.float32)
        acts.append((silu(gate) * up).astype(jnp.bfloat16))
    copies[4].wait()
    copies[5].wait()
    for k in range(n_y):
        columns = slice(k * lanes, (k + 1) * lanes)
        terms = jnp.dot(acts[0], down_ref[:, columns], preferred_element_type=jnp.float32)
        terms = terms + jnp.dot(
            acts[1], other_down_ref[:, columns], preferred_element_type=jnp.float32
        )
        terms = terms.astype(jnp.bfloat16)
        out_ref[k, :n_rows] = terms[:, :feat]
        out_ref[k, n_rows : 2 * n_rows] = terms[:, feat:]


def run_expert(gathered, gain, weights, n_rows, feat):
    n_y, rows_in, lanes = gathered.shape
    at_expert = rows_in - n_rows
    whole = pl.BlockSpec(memory_space=pltpu.VMEM)
    return pl.pallas_call(
        expert_kernel,
        out_shape=(
            jax.ShapeDtypeStruct((n_y, 2 * n_rows + at_expert, feat), jnp.bfloat16),
            jax.ShapeDtypeStruct((4, lanes), jnp.float32),
        ),
        in_specs=[whole, whole] + [pl.BlockSpec(memory_space=pltpu.HBM)] * 6,
        out_specs=(whole, whole),
        scratch_shapes=[pltpu.VMEM((n_rows, gain.shape[0]), jnp.bfloat16)]
        + [pltpu.VMEM(weights[k].shape, jnp.bfloat16) for k in range(6)]
        + [pltpu.SemaphoreType.DMA((6,))],
        compiler_params=pltpu.CompilerParams(vmem_limit_bytes=52 * 2**20),
        name="expert",
    )(gathered, gain, *weights)


def exchange(array, axis):
    return lax.all_to_all(array, axis, 0, 0, tiled=True)


def to_pair(value):
    high = lax.reduce_precision(value, 8, 7)
    return high.astype(jnp.bfloat16), (value - high).astype(jnp.bfloat16)


def round_up(count, unit=8):
    return -(-count // unit) * unit


def sum_lead(array):
    return jnp.sum(array.astype(jnp.float32), axis=0)


def local(
    stream,
    norm_gain_mix,
    query_weight,
    key_weight,
    value_weight,
    score_offset,
    cache_keys,
    cache_values,
    lengths,
    out_weight,
    norm_gain_ffn,
    group_weight,
    router_weight,
    routing,
    expert_gate,
    expert_up,
    expert_down,
    branch_gate,
    dense_gate,
    dense_up,
    dense_down,
):
    seq_count = stream.shape[0]
    width = stream.shape[1]
    n_tp = lax.axis_size(TP)
    n_ep = lax.axis_size("ep")
    n_y = lax.axis_size("y")
    n_core = lax.axis_size("core")
    core = lax.axis_index("core")
    feat = width // n_tp
    offset = lax.axis_index(TP) * feat
    wide = n_core * feat
    wide_offset = lax.axis_index("y") * wide

    swap = [(0, 1), (1, 0)]
    with jax.named_scope("swap_gate"):
        other_gate = lax.ppermute(expert_gate[0], "core", swap)
    with jax.named_scope("swap_up"):
        other_up = lax.ppermute(expert_up[0], "core", swap)
    with jax.named_scope("swap_down"):
        other_down = lax.ppermute(expert_down[0], "core", swap)
    with jax.named_scope("dense_gather"):
        dense_pair = lax.all_gather(
            jnp.concatenate([dense_gate, dense_up, dense_down], 1), "core"
        )
    units = dense_gate.shape[1]
    dense_in = dense_pair[:, :, : 2 * units]
    dense_out = dense_pair[:, :, 2 * units :]
    rows_pad = round_up(seq_count)

    terms, fresh_keys, fresh_values = attend(
        stream,
        norm_gain_mix,
        query_weight,
        key_weight,
        value_weight,
        score_offset,
        cache_keys,
        cache_values,
        lengths,
        out_weight,
        n_tp,
        rows_pad,
    )
    attn = sum_lead(exchange(terms, TP))[:seq_count]

    residual = (
        lax.dynamic_slice_in_dim(stream, offset, feat, 1).astype(jnp.float32)
        + attn.astype(jnp.bfloat16).astype(jnp.float32)
    ).astype(jnp.bfloat16)
    residual_own = residual.astype(jnp.float32)
    pair = lax.all_gather(residual, "core", axis=1, tiled=True)

    experts = router_weight.shape[1]
    groups = group_weight.shape[1]
    per_group = experts // groups
    top = routing.shape[1]
    cap = 2 * ((seq_count + experts - 1) // experts)
    expert_iota = lax.broadcasted_iota(jnp.int32, (1, experts), 1)
    pair_expert = routing.reshape(seq_count * top)
    onehot = (pair_expert[:, None] == expert_iota).astype(jnp.int32)
    before = jnp.cumsum(onehot, 0) - onehot
    slot = jnp.sum(before * onehot, 1)
    index = (pair_expert * cap + slot).reshape(seq_count, top)
    slot_iota = n_core * lax.broadcasted_iota(jnp.int32, (experts, 1, 1), 0) + core
    dispatch = jnp.sum((index[None, :, :] == slot_iota).astype(jnp.int32), 2).astype(jnp.bfloat16)
    send = jnp.dot(dispatch, pair, preferred_element_type=jnp.float32).astype(jnp.bfloat16)

    part = seq_count // n_core
    own_rows = lax.dynamic_slice_in_dim(pair, core * part, part, 0)
    both = seq_count + n_core
    spare = (round_up(both) - seq_count) // n_core
    arrived = exchange(
        jnp.concatenate(
            [
                jnp.broadcast_to(own_rows[None, :, :feat], (n_ep, part, feat)),
                jnp.broadcast_to(own_rows[None, :, feat:], (n_ep, part, feat)),
                jnp.tile(send.reshape(n_ep, n_core, feat), (1, spare, 1)),
            ],
            1,
        ),
        "ep",
    )
    arrived, other_gate, other_up, other_down = lax.optimization_barrier(
        (arrived, other_gate, other_up, other_down)
    )
    total = n_ep * part
    rows = [
        arrived[:, :part].reshape(total, feat).astype(jnp.float32),
        arrived[:, part:seq_count].reshape(total, feat).astype(jnp.float32),
    ]
    picked = arrived[:, seq_count:both].reshape(n_ep, wide)

    home_weights = jnp.concatenate(
        [
            lax.dynamic_slice_in_dim(group_weight, wide_offset, wide, 0),
            lax.dynamic_slice_in_dim(router_weight, wide_offset, wide, 0),
            lax.dynamic_slice_in_dim(branch_gate, wide_offset, wide, 0)[:, None],
        ],
        1,
    )
    products = jnp.dot(pair, home_weights, preferred_element_type=jnp.float32)
    expert_part = products[:, groups : groups + experts]
    home_part = jnp.concatenate(
        [products[:, :groups]]
        + [
            jnp.sum(jnp.where(expert_iota == routing[:, k : k + 1], expert_part, 0.0), 1, keepdims=True)
            for k in range(top)
        ]
        + [products[:, groups + experts :], jnp.sum(jnp.square(pair.astype(jnp.float32)), 1, keepdims=True)],
        1,
    )
    home_count = home_part.shape[1]

    gain_ffn = norm_gain_ffn.astype(jnp.float32)
    gain_wide = lax.dynamic_slice_in_dim(gain_ffn, wide_offset, wide, 0)
    share = total // n_y
    dense_terms = jnp.zeros((total, 2 * units), jnp.float32)
    for k in range(n_core):
        scaled = (rows[k] * gain_wide[k * feat : (k + 1) * feat]).astype(jnp.bfloat16)
        dense_terms += jnp.dot(scaled, dense_in[k], preferred_element_type=jnp.float32)
    dense_terms = dense_terms.astype(jnp.bfloat16)
    squares_part = sum(jnp.sum(r * r, 1) for r in rows)
    squares_high, squares_low = to_pair(squares_part.reshape(n_y, 1, share))
    home_high, home_low = to_pair(home_part.reshape(1, seq_count * home_count))
    lanes = 2 * units

    def lane_pad(array):
        return jnp.pad(array, [(0, 0)] * (array.ndim - 1) + [(0, lanes - array.shape[-1])])

    home_rows = jnp.concatenate([lane_pad(home_high), lane_pad(home_low)], 0)
    gathered = exchange(
        jnp.concatenate(
            [
                dense_terms.reshape(n_y, share, lanes),
                jnp.broadcast_to(home_rows[None], (n_y, *home_rows.shape)),
                lane_pad(squares_high),
                lane_pad(squares_low),
                jnp.broadcast_to(picked[None], (n_y, *picked.shape)),
            ],
            1,
        ),
        "y",
    )

    leaving, sums = run_expert(
        gathered,
        norm_gain_ffn,
        (expert_gate[0], expert_up[0], expert_down[0], other_gate, other_up, other_down),
        n_ep,
        feat,
    )
    home_sum = (sums[0] + sums[1])[: seq_count * home_count].reshape(seq_count, home_count)

    summed = exchange(leaving, "y")
    at_act = n_core * n_ep
    expert_out = sum_lead(summed[:, :at_act]).astype(jnp.bfloat16)
    acts = summed[:, at_act : at_act + share].reshape(total, units)
    dense_terms_out = [
        jnp.dot(acts, dense_out[k], preferred_element_type=jnp.float32)
        .astype(jnp.bfloat16)
        .reshape(n_ep, part, feat)
        for k in range(n_core)
    ]

    returned = exchange(
        jnp.concatenate(
            dense_terms_out
            + [jnp.moveaxis(expert_out.reshape(n_core, n_ep, feat), 0, 1)] * spare,
            1,
        ),
        "ep",
    )
    inverse_two = lax.rsqrt(home_sum[:, home_count - 1 :] / width + epsilon)
    logits = home_sum[:, : home_count - 1] * inverse_two
    group_exp = jnp.exp(logits[:, :groups])
    group_iota = lax.broadcasted_iota(jnp.int32, (1, groups), 1)
    own_group = jnp.sum(
        jnp.where(group_iota == routing[:, :1] // per_group, group_exp, 0.0), 1, keepdims=True
    )
    group_prob = own_group / jnp.sum(group_exp, 1, keepdims=True)
    chosen_exp = jnp.exp(logits[:, groups : groups + top])
    route_gate = group_prob * chosen_exp / jnp.sum(chosen_exp, 1, keepdims=True)
    branch = jax.nn.sigmoid(logits[:, groups + top :])

    stride = returned.shape[1]
    place = lax.broadcasted_iota(jnp.int32, (1, n_ep * stride), 1)
    block, row = place // stride, place % stride
    sequence = lax.broadcasted_iota(jnp.int32, (rows_pad, 1), 0)
    wanted = jnp.where(
        (sequence < seq_count) & (sequence // part == core), sequence % part, -seq_count
    )
    padded = jnp.pad(index, ((0, rows_pad - seq_count), (0, 0)), constant_values=-1)
    taken = [row == wanted + k * part for k in range(n_core)]
    for which in range(top):
        here = block * n_core + core == padded[:, which : which + 1]
        taken += [here & (row == seq_count + k) for k in range(n_core)]
    taken = lax.optimization_barrier(jnp.concatenate(taken, 0).astype(jnp.bfloat16))
    found = jnp.dot(
        taken, returned.reshape(n_ep * stride, feat), preferred_element_type=jnp.float32
    ).reshape(1 + top, n_core, rows_pad, feat)[:, :, :seq_count]
    mixture = [
        branch * found[0, k]
        + sum(route_gate[:, j : j + 1] * found[1 + j, k] for j in range(top))
        for k in range(n_core)
    ]
    mixture = jnp.sum(lax.all_gather(jnp.concatenate(mixture, 1), "core"), 0)
    mixed = (residual_own + lax.dynamic_slice_in_dim(mixture, core * feat, feat, 1)).astype(
        jnp.bfloat16
    )
    return (mixed, fresh_keys, fresh_values)


def solution(mesh):
    n_ep, n_tp = mesh.devices.shape
    split = Mesh(mesh.devices.reshape(n_ep, n_tp // 2, 2), ("ep", "y", "core"))
    placed = (
        P("ep", None),
        P(),
        P(TP, None),
        P(TP, None),
        P(TP, None),
        P(TP),
        P("ep", TP, None),
        P("ep", TP, None),
        P("ep"),
        P(TP, None),
        P(),
        P(),
        P(),
        P("ep", None),
        P("ep", None, TP),
        P("ep", None, TP),
        P("ep", TP, None),
        P(),
        P(TP, "ep"),
        P(TP, "ep"),
        P("ep", TP),
    )
    return jax.shard_map(
        local,
        mesh=split,
        in_specs=placed,
        out_specs=(P("ep", TP), P("ep", TP), P("ep", TP)),
        check_vma=False,
    )
```

```python
import jax
import jax.numpy as jnp
from jax import lax
from jax.experimental import pallas as pl
from jax.experimental.pallas import tpu as pltpu
from jax.sharding import Mesh, PartitionSpec as P


epsilon = 1e-06
TP = ("y", "core")


def across(left, right):
    return lax.dot_general(
        left, right, (((1,), (1,)), ((), ())), preferred_element_type=jnp.float32
    )


def attend_kernel(
    offset_ref,
    lengths_ref,
    stream_ref,
    gain_ref,
    query_ref,
    key_ref,
    value_ref,
    keys_ref,
    values_ref,
    out_weight_ref,
    terms_ref,
    fresh_keys_ref,
    fresh_values_ref,
):
    count, _ = stream_ref.shape
    head_size, cache_len = keys_ref.shape[1:]
    n_blocks, rows, feat = terms_ref.shape
    stream_f = stream_ref[...].astype(jnp.float32)
    inverse = lax.rsqrt(jnp.mean(stream_f * stream_f, -1, keepdims=True) + epsilon)
    normed = (stream_f * inverse * gain_ref[...].astype(jnp.float32)[None]).astype(jnp.bfloat16)
    queries = across(normed, query_ref[...])
    queries = jnp.concatenate([queries, jnp.zeros((rows - count, head_size), jnp.float32)], 0)
    queries = queries.astype(jnp.bfloat16)
    row = lax.broadcasted_iota(jnp.int32, (rows, 1), 0)
    scores = jnp.zeros((rows, cache_len), jnp.float32)
    for s in range(count):
        each = jnp.dot(queries, keys_ref[s], preferred_element_type=jnp.float32)
        scores = jnp.where(row == s, each, scores)
    scores = scores * head_size ** (-0.5) + offset_ref[0]
    filled = jnp.zeros((rows, 1), jnp.int32)
    for s in range(count):
        filled = jnp.where(row == s, lengths_ref[s], filled)
    inside = lax.broadcasted_iota(jnp.int32, (rows, cache_len), 1) < filled
    tail = jnp.log1p(jnp.exp(-jnp.abs(scores)))
    log_keep = jnp.where(inside, jnp.minimum(-scores, 0.0) - tail, 0.0)
    after = (
        lax.broadcasted_iota(jnp.int32, (cache_len, cache_len), 0)
        > lax.broadcasted_iota(jnp.int32, (cache_len, cache_len), 1)
    ).astype(jnp.float32)
    remain = jnp.dot(
        log_keep, after, precision=lax.Precision.HIGHEST, preferred_element_type=jnp.float32
    )
    weights = jnp.where(inside, jnp.exp(jnp.minimum(scores, 0.0) - tail + remain), 0.0)
    weights = weights.astype(jnp.bfloat16)
    heads_out = jnp.zeros((rows, head_size), jnp.float32)
    for s in range(count):
        heads_out = jnp.where(row == s, across(weights, values_ref[s]), heads_out)
    terms = jnp.dot(
        heads_out.astype(jnp.bfloat16), out_weight_ref[...], preferred_element_type=jnp.float32
    ).astype(jnp.bfloat16)
    for k in range(n_blocks):
        terms_ref[k] = terms[:, k * feat : (k + 1) * feat]
    fresh_keys_ref[...] = across(normed, key_ref[...]).astype(jnp.bfloat16)
    fresh_values_ref[...] = across(normed, value_ref[...]).astype(jnp.bfloat16)


def attend(
    stream, gain, query_w, key_w, value_w, offset, keys, values, lengths, out_weight, n_tp, rows
):
    count, width = stream.shape
    whole = pl.BlockSpec(memory_space=pltpu.VMEM)
    fresh = jax.ShapeDtypeStruct((count, key_w.shape[0]), jnp.bfloat16)
    return pl.pallas_call(
        attend_kernel,
        out_shape=(
            jax.ShapeDtypeStruct((n_tp, rows, width // n_tp), jnp.bfloat16),
            fresh,
            fresh,
        ),
        in_specs=[pl.BlockSpec(memory_space=pltpu.SMEM)] * 2 + [whole] * 8,
        out_specs=(whole, whole, whole),
        name="attend",
    )(offset, lengths, stream, gain, query_w, key_w, value_w, keys, values, out_weight)


def spread_kernel(arrived_ref, gain_ref, dense_in_ref, home_ref, out_ref, wide_ref, rows_ref, block_ref):
    n_ep, _, feat = arrived_ref.shape
    n_y, rows_out, lanes = out_ref.shape
    at_expert = rows_out - n_ep
    share = at_expert - 4
    total = n_y * share
    part = total // n_ep
    wide_ref[...] = arrived_ref[...].astype(jnp.float32)
    for b in range(n_ep):
        for k in range(2):
            rows_ref[k, pl.ds(b * part, part)] = wide_ref[b, pl.ds(k * part, part)]
            rows_ref[k, pl.ds(total + b, 1)] = wide_ref[b, pl.ds(2 * part + k, 1)]
    products = jnp.zeros((total, lanes), jnp.float32)
    squares = jnp.zeros((total, 1), jnp.float32)
    for k in range(2):
        rows = rows_ref[k, :total]
        squares = squares + jnp.sum(rows * rows, 1, keepdims=True)
        gain = gain_ref[:, k * feat : (k + 1) * feat].astype(jnp.float32)
        products = products + jnp.dot(
            (rows * gain).astype(jnp.bfloat16),
            dense_in_ref[k, :, :lanes],
            preferred_element_type=jnp.float32,
        )
        picked = rows_ref[k, pl.ds(total, n_ep)].astype(jnp.bfloat16)
        for y in range(n_y):
            out_ref[y, at_expert:, k * feat : (k + 1) * feat] = picked
    diagonal = lax.broadcasted_iota(jnp.int32, (share, lanes), 0) == lax.broadcasted_iota(
        jnp.int32, (share, lanes), 1
    )
    for y in range(n_y):
        part_squares = squares[y * share : (y + 1) * share]
        line = jnp.sum(jnp.where(diagonal, part_squares, 0.0), 0, keepdims=True)
        high = line.astype(jnp.bfloat16).astype(jnp.float32)
        block_ref[y, pl.ds(0, share)] = products[y * share : (y + 1) * share]
        block_ref[y, pl.ds(share, 2)] = home_ref[...]
        block_ref[y, pl.ds(share + 2, 1)] = high
        block_ref[y, pl.ds(share + 3, 1)] = line - high
        out_ref[y, :at_expert] = block_ref[y].astype(jnp.bfloat16)


def spread(arrived, gain, dense_in, home, n_y, share):
    n_ep, _, feat = arrived.shape
    lanes = home.shape[1]
    whole = pl.BlockSpec(memory_space=pltpu.VMEM)
    return pl.pallas_call(
        spread_kernel,
        out_shape=jax.ShapeDtypeStruct((n_y, share + 4 + n_ep, lanes), jnp.bfloat16),
        in_specs=[whole] * 4,
        out_specs=whole,
        scratch_shapes=[
            pltpu.VMEM(arrived.shape, jnp.float32),
            pltpu.VMEM((2, n_y * share + n_ep, feat), jnp.float32),
            pltpu.VMEM((n_y, share + 4, lanes), jnp.float32),
        ],
        compiler_params=pltpu.CompilerParams(vmem_limit_bytes=52 * 2**20),
        name="spread",
    )(arrived, gain, dense_in, home)


def silu(value):
    return value * jax.nn.sigmoid(value)


def expert_kernel(
    gathered_ref,
    gain_ref,
    gate_hbm,
    up_hbm,
    down_hbm,
    other_gate_hbm,
    other_up_hbm,
    other_down_hbm,
    out_ref,
    home_ref,
    hidden_ref,
    gate_ref,
    up_ref,
    down_ref,
    other_gate_ref,
    other_up_ref,
    other_down_ref,
    sems,
):
    copies = [
        pltpu.make_async_copy(source, target, sems.at[k])
        for k, (source, target) in enumerate(
            (
                (gate_hbm, gate_ref),
                (up_hbm, up_ref),
                (other_gate_hbm, other_gate_ref),
                (other_up_hbm, other_up_ref),
                (down_hbm, down_ref),
                (other_down_hbm, other_down_ref),
            )
        )
    ]
    for copy in copies:
        copy.start()
    n_y, rows_in, lanes = gathered_ref.shape
    n_rows, width = hidden_ref.shape
    feat = out_ref.shape[2]
    units = lanes // 2
    at_expert = rows_in - n_rows
    share = at_expert - 4

    both = gathered_ref[0, :at_expert].astype(jnp.float32)
    for k in range(1, n_y):
        both = both + gathered_ref[k, :at_expert].astype(jnp.float32)
    home_ref[...] = both[share:]
    squares = both[share + 2 : share + 3] + both[share + 3 : share + 4]
    diagonal = lax.broadcasted_iota(jnp.int32, (at_expert, lanes), 0) == lax.broadcasted_iota(
        jnp.int32, (at_expert, lanes), 1
    )
    column = jnp.sum(jnp.where(diagonal, squares, 0.0), 1, keepdims=True)
    both = both * lax.rsqrt(column / width + epsilon)
    act = (silu(both[:, :units]) * both[:, units:]).astype(jnp.bfloat16)
    for k in range(n_y):
        out_ref[k, 2 * n_rows :] = act

    squares = jnp.zeros((n_rows, 1), jnp.float32)
    for k in range(n_y):
        rows = gathered_ref[k, at_expert:].astype(jnp.float32)
        squares = squares + jnp.sum(rows * rows, 1, keepdims=True)
    inverse = lax.rsqrt(squares / width + epsilon)
    for k in range(n_y):
        rows = gathered_ref[k, at_expert:].astype(jnp.float32)
        gain = gain_ref[pl.ds(k * lanes, lanes)].astype(jnp.float32)[None]
        hidden_ref[:, k * lanes : (k + 1) * lanes] = (rows * inverse * gain).astype(jnp.bfloat16)
    hidden_in = hidden_ref[...]
    acts = []
    for k, (gate_w, up_w) in enumerate(((gate_ref, up_ref), (other_gate_ref, other_up_ref))):
        copies[2 * k].wait()
        gate = jnp.dot(hidden_in, gate_w[...], preferred_element_type=jnp.float32)
        copies[2 * k + 1].wait()
        up = jnp.dot(hidden_in, up_w[...], preferred_element_type=jnp.float32)
        acts.append((silu(gate) * up).astype(jnp.bfloat16))
    copies[4].wait()
    copies[5].wait()
    for k in range(n_y):
        columns = slice(k * lanes, (k + 1) * lanes)
        terms = jnp.dot(acts[0], down_ref[:, columns], preferred_element_type=jnp.float32)
        terms = terms + jnp.dot(
            acts[1], other_down_ref[:, columns], preferred_element_type=jnp.float32
        )
        terms = terms.astype(jnp.bfloat16)
        out_ref[k, :n_rows] = terms[:, :feat]
        out_ref[k, n_rows : 2 * n_rows] = terms[:, feat:]


def run_expert(gathered, gain, weights, n_rows, feat):
    n_y, rows_in, lanes = gathered.shape
    at_expert = rows_in - n_rows
    whole = pl.BlockSpec(memory_space=pltpu.VMEM)
    return pl.pallas_call(
        expert_kernel,
        out_shape=(
            jax.ShapeDtypeStruct((n_y, 2 * n_rows + at_expert, feat), jnp.bfloat16),
            jax.ShapeDtypeStruct((4, lanes), jnp.float32),
        ),
        in_specs=[whole, whole] + [pl.BlockSpec(memory_space=pltpu.HBM)] * 6,
        out_specs=(whole, whole),
        scratch_shapes=[pltpu.VMEM((n_rows, gain.shape[0]), jnp.bfloat16)]
        + [pltpu.VMEM(weights[k].shape, jnp.bfloat16) for k in range(6)]
        + [pltpu.SemaphoreType.DMA((6,))],
        compiler_params=pltpu.CompilerParams(vmem_limit_bytes=52 * 2**20),
        name="expert",
    )(gathered, gain, *weights)


def exchange(array, axis):
    return lax.all_to_all(array, axis, 0, 0, tiled=True)


def round_up(count, unit=8):
    return -(-count // unit) * unit


def sum_lead(array):
    return jnp.sum(array.astype(jnp.float32), axis=0)


def local(
    stream,
    norm_gain_mix,
    query_weight,
    key_weight,
    value_weight,
    score_offset,
    cache_keys,
    cache_values,
    lengths,
    out_weight,
    norm_gain_ffn,
    group_weight,
    router_weight,
    routing,
    expert_gate,
    expert_up,
    expert_down,
    branch_gate,
    dense_gate,
    dense_up,
    dense_down,
):
    seq_count = stream.shape[0]
    width = stream.shape[1]
    n_tp = lax.axis_size(TP)
    n_ep = lax.axis_size("ep")
    n_y = lax.axis_size("y")
    n_core = lax.axis_size("core")
    core = lax.axis_index("core")
    feat = width // n_tp
    offset = lax.axis_index(TP) * feat
    wide = n_core * feat
    wide_offset = lax.axis_index("y") * wide

    swap = [(0, 1), (1, 0)]
    other_gate = lax.ppermute(expert_gate[0], "core", swap)
    other_up = lax.ppermute(expert_up[0], "core", swap)
    other_down = lax.ppermute(expert_down[0], "core", swap)
    dense_pair = lax.all_gather(
        jnp.concatenate([dense_gate, dense_up, dense_down], 1), "core"
    )
    units = dense_gate.shape[1]
    dense_out = dense_pair[:, :, 2 * units :]
    rows_pad = round_up(seq_count)

    terms, fresh_keys, fresh_values = attend(
        stream,
        norm_gain_mix,
        query_weight,
        key_weight,
        value_weight,
        score_offset,
        cache_keys,
        cache_values,
        lengths,
        out_weight,
        n_tp,
        rows_pad,
    )
    attn = sum_lead(exchange(terms, TP))[:seq_count]

    residual = (
        lax.dynamic_slice_in_dim(stream, offset, feat, 1).astype(jnp.float32)
        + attn.astype(jnp.bfloat16).astype(jnp.float32)
    ).astype(jnp.bfloat16)
    residual_own = residual.astype(jnp.float32)
    pair = lax.all_gather(residual, "core", axis=1, tiled=True)

    experts = router_weight.shape[1]
    groups = group_weight.shape[1]
    per_group = experts // groups
    top = routing.shape[1]
    cap = 2 * ((seq_count + experts - 1) // experts)
    expert_iota = lax.broadcasted_iota(jnp.int32, (1, experts), 1)
    pair_expert = routing.reshape(seq_count * top)
    onehot = (pair_expert[:, None] == expert_iota).astype(jnp.int32)
    before = jnp.cumsum(onehot, 0) - onehot
    slot = jnp.sum(before * onehot, 1)
    index = (pair_expert * cap + slot).reshape(seq_count, top)
    slot_iota = n_core * lax.broadcasted_iota(jnp.int32, (experts, 1, 1), 0) + core
    dispatch = jnp.sum((index[None, :, :] == slot_iota).astype(jnp.int32), 2).astype(jnp.bfloat16)
    send = jnp.dot(dispatch, pair, preferred_element_type=jnp.float32).astype(jnp.bfloat16)

    part = seq_count // n_core
    own_rows = lax.dynamic_slice_in_dim(pair, core * part, part, 0)
    both = seq_count + n_core
    spare = (round_up(both) - seq_count) // n_core
    leaving = jnp.concatenate(
        [
            jnp.broadcast_to(own_rows[None, :, :feat], (n_ep, part, feat)),
            jnp.broadcast_to(own_rows[None, :, feat:], (n_ep, part, feat)),
            jnp.tile(send.reshape(n_ep, n_core, feat), (1, spare, 1)),
        ],
        1,
    )
    arrived = exchange(leaving, "ep")
    arrived, other_gate, other_up, other_down = lax.optimization_barrier(
        (arrived, other_gate, other_up, other_down)
    )
    total = n_ep * part
    home_weights = jnp.concatenate(
        [
            lax.dynamic_slice_in_dim(group_weight, wide_offset, wide, 0),
            lax.dynamic_slice_in_dim(router_weight, wide_offset, wide, 0),
            lax.dynamic_slice_in_dim(branch_gate, wide_offset, wide, 0)[:, None],
        ],
        1,
    )
    products = jnp.dot(pair, home_weights, preferred_element_type=jnp.float32)
    expert_part = products[:, groups : groups + experts]
    home_part = jnp.concatenate(
        [products[:, :groups]]
        + [
            jnp.sum(jnp.where(expert_iota == routing[:, k : k + 1], expert_part, 0.0), 1, keepdims=True)
            for k in range(top)
        ]
        + [products[:, groups + experts :], jnp.sum(jnp.square(pair.astype(jnp.float32)), 1, keepdims=True)],
        1,
    )
    home_count = home_part.shape[1]

    gain_wide = lax.dynamic_slice_in_dim(norm_gain_ffn, wide_offset, wide, 0)[None]
    share = total // n_y
    lanes = 2 * units
    flat = jnp.pad(
        home_part.reshape(1, seq_count * home_count), ((0, 0), (0, lanes - seq_count * home_count))
    )
    high = lax.reduce_precision(flat, 8, 7)
    home_rows = jnp.concatenate([high, flat - high], 0)
    leaving = spread(arrived, gain_wide, dense_pair, home_rows, n_y, share)
    gathered = exchange(leaving, "y")

    leaving, sums = run_expert(
        gathered,
        norm_gain_ffn,
        (expert_gate[0], expert_up[0], expert_down[0], other_gate, other_up, other_down),
        n_ep,
        feat,
    )
    home_sum = (sums[0] + sums[1])[: seq_count * home_count].reshape(seq_count, home_count)

    summed = exchange(leaving, "y")
    at_act = n_core * n_ep
    expert_out = sum_lead(summed[:, :at_act]).astype(jnp.bfloat16)
    acts = summed[:, at_act : at_act + share].reshape(total, units)
    dense_terms_out = [
        jnp.dot(acts, dense_out[k], preferred_element_type=jnp.float32)
        .astype(jnp.bfloat16)
        .reshape(n_ep, part, feat)
        for k in range(n_core)
    ]

    returned = exchange(
        jnp.concatenate(
            dense_terms_out
            + [jnp.moveaxis(expert_out.reshape(n_core, n_ep, feat), 0, 1)] * spare,
            1,
        ),
        "ep",
    )
    inverse_two = lax.rsqrt(home_sum[:, home_count - 1 :] / width + epsilon)
    logits = home_sum[:, : home_count - 1] * inverse_two
    group_exp = jnp.exp(logits[:, :groups])
    group_iota = lax.broadcasted_iota(jnp.int32, (1, groups), 1)
    own_group = jnp.sum(
        jnp.where(group_iota == routing[:, :1] // per_group, group_exp, 0.0), 1, keepdims=True
    )
    group_prob = own_group / jnp.sum(group_exp, 1, keepdims=True)
    chosen_exp = jnp.exp(logits[:, groups : groups + top])
    route_gate = group_prob * chosen_exp / jnp.sum(chosen_exp, 1, keepdims=True)
    branch = jax.nn.sigmoid(logits[:, groups + top :])

    stride = returned.shape[1]
    place = lax.broadcasted_iota(jnp.int32, (1, n_ep * stride), 1)
    block, row = place // stride, place % stride
    sequence = lax.broadcasted_iota(jnp.int32, (rows_pad, 1), 0)
    wanted = jnp.where(
        (sequence < seq_count) & (sequence // part == core), sequence % part, -seq_count
    )
    padded = jnp.pad(index, ((0, rows_pad - seq_count), (0, 0)), constant_values=-1)
    taken = [row == wanted + k * part for k in range(n_core)]
    for which in range(top):
        here = block * n_core + core == padded[:, which : which + 1]
        taken += [here & (row == seq_count + k) for k in range(n_core)]
    taken = lax.optimization_barrier(jnp.concatenate(taken, 0).astype(jnp.bfloat16))
    found = jnp.dot(
        taken, returned.reshape(n_ep * stride, feat), preferred_element_type=jnp.float32
    ).reshape(1 + top, n_core, rows_pad, feat)[:, :, :seq_count]
    mixture = [
        branch * found[0, k]
        + sum(route_gate[:, j : j + 1] * found[1 + j, k] for j in range(top))
        for k in range(n_core)
    ]
    mixture = jnp.sum(lax.all_gather(jnp.concatenate(mixture, 1), "core"), 0)
    mixed = (residual_own + lax.dynamic_slice_in_dim(mixture, core * feat, feat, 1)).astype(
        jnp.bfloat16
    )
    return (mixed, fresh_keys, fresh_values)


def solution(mesh):
    n_ep, n_tp = mesh.devices.shape
    split = Mesh(mesh.devices.reshape(n_ep, n_tp // 2, 2), ("ep", "y", "core"))
    placed = (
        P("ep", None),
        P(),
        P(TP, None),
        P(TP, None),
        P(TP, None),
        P(TP),
        P("ep", TP, None),
        P("ep", TP, None),
        P("ep"),
        P(TP, None),
        P(),
        P(),
        P(),
        P("ep", None),
        P("ep", None, TP),
        P("ep", None, TP),
        P("ep", TP, None),
        P(),
        P(TP, "ep"),
        P(TP, "ep"),
        P("ep", TP),
    )
    return jax.shard_map(
        local,
        mesh=split,
        in_specs=placed,
        out_specs=(P("ep", TP), P("ep", TP), P("ep", TP)),
        check_vma=False,
    )
```

```python
import jax
import jax.numpy as jnp
from jax import lax
from jax.experimental import pallas as pl
from jax.experimental.pallas import tpu as pltpu
from jax.sharding import Mesh, PartitionSpec as P


epsilon = 1e-06
TP = ("y", "core")


def across(left, right):
    return lax.dot_general(
        left, right, (((1,), (1,)), ((), ())), preferred_element_type=jnp.float32
    )


def attend_kernel(
    offset_ref,
    lengths_ref,
    stream_ref,
    gain_ref,
    query_ref,
    keys_hbm,
    values_hbm,
    out_weight_hbm,
    terms_ref,
    normed_ref,
    keys_ref,
    values_ref,
    out_weight_ref,
    sems,
):
    copies = [
        pltpu.make_async_copy(source, target, sems.at[k])
        for k, (source, target) in enumerate(
            (
                (keys_hbm, keys_ref),
                (values_hbm, values_ref),
                (out_weight_hbm, out_weight_ref),
            )
        )
    ]
    for copy in copies:
        copy.start()
    count, _ = stream_ref.shape
    head_size, cache_len = keys_ref.shape[1:]
    n_blocks, rows, feat = terms_ref.shape
    stream_f = stream_ref[...].astype(jnp.float32)
    inverse = lax.rsqrt(jnp.mean(stream_f * stream_f, -1, keepdims=True) + epsilon)
    normed = (stream_f * inverse * gain_ref[...].astype(jnp.float32)[None]).astype(jnp.bfloat16)
    normed_ref[...] = normed
    queries = across(normed, query_ref[...])
    queries = jnp.concatenate([queries, jnp.zeros((rows - count, head_size), jnp.float32)], 0)
    queries = queries.astype(jnp.bfloat16)
    row = lax.broadcasted_iota(jnp.int32, (rows, 1), 0)
    after = (
        lax.broadcasted_iota(jnp.int32, (cache_len, cache_len), 0)
        > lax.broadcasted_iota(jnp.int32, (cache_len, cache_len), 1)
    ).astype(jnp.float32)
    copies[0].wait()
    scores = jnp.zeros((rows, cache_len), jnp.float32)
    for s in range(count):
        each = jnp.dot(queries, keys_ref[s], preferred_element_type=jnp.float32)
        scores = jnp.where(row == s, each, scores)
    scores = scores * head_size ** (-0.5) + offset_ref[0]
    filled = jnp.zeros((rows, 1), jnp.int32)
    for s in range(count):
        filled = jnp.where(row == s, lengths_ref[s], filled)
    inside = lax.broadcasted_iota(jnp.int32, (rows, cache_len), 1) < filled
    tail = jnp.log1p(jnp.exp(-jnp.abs(scores)))
    log_keep = jnp.where(inside, jnp.minimum(-scores, 0.0) - tail, 0.0)
    remain = jnp.dot(
        log_keep, after, precision=lax.Precision.HIGHEST, preferred_element_type=jnp.float32
    )
    weights = jnp.where(inside, jnp.exp(jnp.minimum(scores, 0.0) - tail + remain), 0.0)
    weights = weights.astype(jnp.bfloat16)
    copies[1].wait()
    heads_out = jnp.zeros((rows, head_size), jnp.float32)
    for s in range(count):
        heads_out = jnp.where(row == s, across(weights, values_ref[s]), heads_out)
    copies[2].wait()
    terms = jnp.dot(
        heads_out.astype(jnp.bfloat16), out_weight_ref[...], preferred_element_type=jnp.float32
    ).astype(jnp.bfloat16)
    for k in range(n_blocks):
        terms_ref[k] = terms[:, k * feat : (k + 1) * feat]


def attend(stream, gain, query_w, offset, keys, values, lengths, out_weight, n_tp, rows):
    count, width = stream.shape
    whole = pl.BlockSpec(memory_space=pltpu.VMEM)
    return pl.pallas_call(
        attend_kernel,
        out_shape=(
            jax.ShapeDtypeStruct((n_tp, rows, width // n_tp), jnp.bfloat16),
            jax.ShapeDtypeStruct((count, width), jnp.bfloat16),
        ),
        in_specs=[pl.BlockSpec(memory_space=pltpu.SMEM)] * 2
        + [whole] * 3
        + [pl.BlockSpec(memory_space=pltpu.HBM)] * 3,
        out_specs=(whole, whole),
        scratch_shapes=[
            pltpu.VMEM(each.shape, jnp.bfloat16) for each in (keys, values, out_weight)
        ]
        + [pltpu.SemaphoreType.DMA((3,))],
        name="attend",
    )(offset, lengths, stream, gain, query_w, keys, values, out_weight)


def pack_kernel(core_ref, pair_ref, dispatch_ref, out_ref, send_ref):
    n_ep, stride, feat = out_ref.shape
    part = pair_ref.shape[0] // 2
    pair = pair_ref[...]
    send_ref[:n_ep] = jnp.dot(dispatch_ref[...], pair, preferred_element_type=jnp.float32)
    pair = pair.astype(jnp.float32)
    mine = jnp.where(core_ref[0] == 0, pair[:part], pair[part:])
    rest = jnp.zeros((stride - 2 * part, feat), jnp.float32)
    base = jnp.concatenate([mine[:, :feat], mine[:, feat:], rest], 0)
    row = lax.broadcasted_iota(jnp.int32, (stride, 1), 0)
    for b in range(n_ep):
        block = jnp.where(row == 2 * part, send_ref[pl.ds(b, 1), :feat], base)
        block = jnp.where(row == 2 * part + 1, send_ref[pl.ds(b, 1), feat:], block)
        out_ref[b] = block.astype(jnp.bfloat16)


def pack(core, pair, dispatch, stride):
    n_ep = dispatch.shape[0]
    wide = pair.shape[1]
    whole = pl.BlockSpec(memory_space=pltpu.VMEM)
    return pl.pallas_call(
        pack_kernel,
        out_shape=jax.ShapeDtypeStruct((n_ep, stride, wide // 2), jnp.bfloat16),
        in_specs=[pl.BlockSpec(memory_space=pltpu.SMEM), whole, whole],
        out_specs=whole,
        scratch_shapes=[pltpu.VMEM((n_ep + guard, wide), jnp.float32)],
        compiler_params=pltpu.CompilerParams(vmem_limit_bytes=52 * 2**20),
        name="pack",
    )(core, pair, dispatch)


def merge_kernel(summed_ref, dense_out_ref, out_ref, act_ref, dense_ref, expert_ref, block_ref):
    n_ep, stride, feat = out_ref.shape
    n_y, _, _ = summed_ref.shape
    at_act = 2 * n_ep
    total = act_ref.shape[0] - guard
    share = total // n_y
    part = total // n_ep
    expert = jnp.zeros((at_act, feat), jnp.float32)
    for y in range(n_y):
        expert = expert + summed_ref[y, :at_act].astype(jnp.float32)
        act_ref[pl.ds(y * share, share)] = summed_ref[y, at_act:].astype(jnp.float32)[:share]
    expert_ref[:at_act] = expert
    acts = act_ref[:total].astype(jnp.bfloat16)
    for k in range(2):
        dense_ref[k, :total] = jnp.dot(
            acts, dense_out_ref[k, :, 2 * feat :], preferred_element_type=jnp.float32
        )
    block_ref[...] = jnp.zeros_like(block_ref)
    for b in range(n_ep):
        for k in range(2):
            block_ref[b, pl.ds(k * part, part)] = dense_ref[k, pl.ds(b * part, part)]
            block_ref[b, pl.ds(2 * part + k, 1)] = expert_ref[pl.ds(k * n_ep + b, 1)]
    out_ref[...] = block_ref[:, :stride].astype(jnp.bfloat16)


def merge(summed, dense_pair, n_ep, stride, part):
    feat = summed.shape[2]
    total = n_ep * part
    whole = pl.BlockSpec(memory_space=pltpu.VMEM)
    return pl.pallas_call(
        merge_kernel,
        out_shape=jax.ShapeDtypeStruct((n_ep, stride, feat), jnp.bfloat16),
        in_specs=[whole, whole],
        out_specs=whole,
        scratch_shapes=[
            pltpu.VMEM((total + guard, feat), jnp.float32),
            pltpu.VMEM((2, total + guard, feat), jnp.float32),
            pltpu.VMEM((2 * n_ep + guard, feat), jnp.float32),
            pltpu.VMEM((n_ep, stride + guard, feat), jnp.float32),
        ],
        compiler_params=pltpu.CompilerParams(vmem_limit_bytes=52 * 2**20),
        name="merge",
    )(summed, dense_pair)


def spread_kernel(arrived_ref, gain_ref, dense_in_ref, home_ref, out_ref, wide_ref, rows_ref, block_ref):
    n_ep, stride, feat = arrived_ref.shape
    n_y, rows_out, lanes = out_ref.shape
    at_expert = rows_out - n_ep
    share = at_expert - 4
    total = n_y * share
    part = total // n_ep
    wide_ref[:, :stride] = arrived_ref[...].astype(jnp.float32)
    for b in range(n_ep):
        for k in range(2):
            rows_ref[k, pl.ds(b * part, part)] = wide_ref[b, pl.ds(k * part, part)]
            rows_ref[k, pl.ds(total + b, 1)] = wide_ref[b, pl.ds(2 * part + k, 1)]
    products = jnp.zeros((total, lanes), jnp.float32)
    squares = jnp.zeros((total, 1), jnp.float32)
    for k in range(2):
        rows = rows_ref[k, :total]
        squares = squares + jnp.sum(rows * rows, 1, keepdims=True)
        gain = gain_ref[:, k * feat : (k + 1) * feat].astype(jnp.float32)
        products = products + jnp.dot(
            (rows * gain).astype(jnp.bfloat16),
            dense_in_ref[k, :, :lanes],
            preferred_element_type=jnp.float32,
        )
        picked = rows_ref[k, pl.ds(total, n_ep)].astype(jnp.bfloat16)
        for y in range(n_y):
            out_ref[y, at_expert:, k * feat : (k + 1) * feat] = picked
    diagonal = lax.broadcasted_iota(jnp.int32, (share, lanes), 0) == lax.broadcasted_iota(
        jnp.int32, (share, lanes), 1
    )
    for y in range(n_y):
        part_squares = squares[y * share : (y + 1) * share]
        line = jnp.sum(jnp.where(diagonal, part_squares, 0.0), 0, keepdims=True)
        high = line.astype(jnp.bfloat16).astype(jnp.float32)
        block_ref[y, pl.ds(0, share)] = products[y * share : (y + 1) * share]
        block_ref[y, pl.ds(share, 2)] = home_ref[...]
        block_ref[y, pl.ds(share + 2, 1)] = high
        block_ref[y, pl.ds(share + 3, 1)] = line - high
        out_ref[y, :at_expert] = block_ref[y, :at_expert].astype(jnp.bfloat16)


def spread(arrived, gain, dense_in, home, n_y, share):
    n_ep, stride, feat = arrived.shape
    lanes = home.shape[1]
    whole = pl.BlockSpec(memory_space=pltpu.VMEM)
    return pl.pallas_call(
        spread_kernel,
        out_shape=jax.ShapeDtypeStruct((n_y, share + 4 + n_ep, lanes), jnp.bfloat16),
        in_specs=[whole] * 4,
        out_specs=whole,
        scratch_shapes=[
            pltpu.VMEM((n_ep, stride + guard, feat), jnp.float32),
            pltpu.VMEM((2, n_y * share + n_ep + guard, feat), jnp.float32),
            pltpu.VMEM((n_y, share + 4 + guard, lanes), jnp.float32),
        ],
        compiler_params=pltpu.CompilerParams(vmem_limit_bytes=52 * 2**20),
        name="spread",
    )(arrived, gain, dense_in, home)


guard = 8


def silu(value):
    return value * jax.nn.sigmoid(value)


def expert_kernel(
    gathered_ref,
    gain_ref,
    gate_hbm,
    up_hbm,
    down_hbm,
    other_gate_hbm,
    other_up_hbm,
    other_down_hbm,
    out_ref,
    home_ref,
    hidden_ref,
    gate_ref,
    up_ref,
    down_ref,
    other_gate_ref,
    other_up_ref,
    other_down_ref,
    sems,
):
    copies = [
        pltpu.make_async_copy(source, target, sems.at[k])
        for k, (source, target) in enumerate(
            (
                (gate_hbm, gate_ref),
                (up_hbm, up_ref),
                (other_gate_hbm, other_gate_ref),
                (other_up_hbm, other_up_ref),
                (down_hbm, down_ref),
                (other_down_hbm, other_down_ref),
            )
        )
    ]
    for copy in copies:
        copy.start()
    n_y, rows_in, lanes = gathered_ref.shape
    n_rows, width = hidden_ref.shape
    feat = out_ref.shape[2]
    units = lanes // 2
    at_expert = rows_in - n_rows
    share = at_expert - 4

    both = gathered_ref[0, :at_expert].astype(jnp.float32)
    for k in range(1, n_y):
        both = both + gathered_ref[k, :at_expert].astype(jnp.float32)
    home_ref[...] = both[share:]
    squares = both[share + 2 : share + 3] + both[share + 3 : share + 4]
    diagonal = lax.broadcasted_iota(jnp.int32, (at_expert, lanes), 0) == lax.broadcasted_iota(
        jnp.int32, (at_expert, lanes), 1
    )
    column = jnp.sum(jnp.where(diagonal, squares, 0.0), 1, keepdims=True)
    both = both * lax.rsqrt(column / width + epsilon)
    act = (silu(both[:, :units]) * both[:, units:]).astype(jnp.bfloat16)
    for k in range(n_y):
        out_ref[k, 2 * n_rows :] = act

    squares = jnp.zeros((n_rows, 1), jnp.float32)
    for k in range(n_y):
        rows = gathered_ref[k, at_expert:].astype(jnp.float32)
        squares = squares + jnp.sum(rows * rows, 1, keepdims=True)
    inverse = lax.rsqrt(squares / width + epsilon)
    for k in range(n_y):
        rows = gathered_ref[k, at_expert:].astype(jnp.float32)
        gain = gain_ref[pl.ds(k * lanes, lanes)].astype(jnp.float32)[None]
        hidden_ref[:, k * lanes : (k + 1) * lanes] = (rows * inverse * gain).astype(jnp.bfloat16)
    hidden_in = hidden_ref[...]
    acts = []
    for k, (gate_w, up_w) in enumerate(((gate_ref, up_ref), (other_gate_ref, other_up_ref))):
        copies[2 * k].wait()
        gate = jnp.dot(hidden_in, gate_w[...], preferred_element_type=jnp.float32)
        copies[2 * k + 1].wait()
        up = jnp.dot(hidden_in, up_w[...], preferred_element_type=jnp.float32)
        acts.append((silu(gate) * up).astype(jnp.bfloat16))
    copies[4].wait()
    copies[5].wait()
    for k in range(n_y):
        columns = slice(k * lanes, (k + 1) * lanes)
        terms = jnp.dot(acts[0], down_ref[:, columns], preferred_element_type=jnp.float32)
        terms = terms + jnp.dot(
            acts[1], other_down_ref[:, columns], preferred_element_type=jnp.float32
        )
        terms = terms.astype(jnp.bfloat16)
        out_ref[k, :n_rows] = terms[:, :feat]
        out_ref[k, n_rows : 2 * n_rows] = terms[:, feat:]


def run_expert(gathered, gain, weights, n_rows, feat):
    n_y, rows_in, lanes = gathered.shape
    at_expert = rows_in - n_rows
    whole = pl.BlockSpec(memory_space=pltpu.VMEM)
    return pl.pallas_call(
        expert_kernel,
        out_shape=(
            jax.ShapeDtypeStruct((n_y, 2 * n_rows + at_expert, feat), jnp.bfloat16),
            jax.ShapeDtypeStruct((4, lanes), jnp.float32),
        ),
        in_specs=[whole, whole] + [pl.BlockSpec(memory_space=pltpu.HBM)] * 6,
        out_specs=(whole, whole),
        scratch_shapes=[pltpu.VMEM((n_rows, gain.shape[0]), jnp.bfloat16)]
        + [pltpu.VMEM(weights[k].shape, jnp.bfloat16) for k in range(6)]
        + [pltpu.SemaphoreType.DMA((6,))],
        compiler_params=pltpu.CompilerParams(vmem_limit_bytes=52 * 2**20),
        name="expert",
    )(gathered, gain, *weights)


def exchange(array, axis):
    return lax.all_to_all(array, axis, 0, 0, tiled=True)


def round_up(count, unit=8):
    return -(-count // unit) * unit


def sum_lead(array):
    return jnp.sum(array.astype(jnp.float32), axis=0)


def local(
    stream,
    norm_gain_mix,
    query_weight,
    key_weight,
    value_weight,
    score_offset,
    cache_keys,
    cache_values,
    lengths,
    out_weight,
    norm_gain_ffn,
    group_weight,
    router_weight,
    routing,
    expert_gate,
    expert_up,
    expert_down,
    branch_gate,
    dense_gate,
    dense_up,
    dense_down,
):
    seq_count = stream.shape[0]
    width = stream.shape[1]
    n_tp = lax.axis_size(TP)
    n_ep = lax.axis_size("ep")
    n_y = lax.axis_size("y")
    n_core = lax.axis_size("core")
    core = lax.axis_index("core")
    feat = width // n_tp
    offset = lax.axis_index(TP) * feat
    wide = n_core * feat
    wide_offset = lax.axis_index("y") * wide

    swap = [(0, 1), (1, 0)]
    other_gate = lax.ppermute(expert_gate[0], "core", swap)
    other_up = lax.ppermute(expert_up[0], "core", swap)
    other_down = lax.ppermute(expert_down[0], "core", swap)
    dense_pair = lax.all_gather(
        jnp.concatenate([dense_gate, dense_up, dense_down], 1), "core"
    )
    units = dense_gate.shape[1]
    rows_pad = round_up(seq_count)

    stream_own = lax.optimization_barrier(
        lax.dynamic_slice_in_dim(stream, offset, feat, 1).astype(jnp.float32)
    )
    terms, normed = attend(
        stream,
        norm_gain_mix,
        query_weight,
        score_offset,
        cache_keys,
        cache_values,
        lengths,
        out_weight,
        n_tp,
        rows_pad,
    )
    attn = sum_lead(exchange(terms, TP))[:seq_count]

    residual = (
        stream_own
        + attn.astype(jnp.bfloat16).astype(jnp.float32)
    ).astype(jnp.bfloat16)
    residual_own = residual.astype(jnp.float32)
    pair = lax.all_gather(residual, "core", axis=1, tiled=True)

    experts = router_weight.shape[1]
    groups = group_weight.shape[1]
    per_group = experts // groups
    top = routing.shape[1]
    cap = 2 * ((seq_count + experts - 1) // experts)
    expert_iota = lax.broadcasted_iota(jnp.int32, (1, experts), 1)
    pair_expert = routing.reshape(seq_count * top)
    onehot = (pair_expert[:, None] == expert_iota).astype(jnp.int32)
    before = jnp.cumsum(onehot, 0) - onehot
    slot = jnp.sum(before * onehot, 1)
    index = (pair_expert * cap + slot).reshape(seq_count, top)
    slot_iota = n_core * lax.broadcasted_iota(jnp.int32, (experts, 1, 1), 0) + core
    dispatch = jnp.sum((index[None, :, :] == slot_iota).astype(jnp.int32), 2).astype(jnp.bfloat16)

    part = seq_count // n_core
    stride = round_up(seq_count + n_core)
    leaving = pack(core[None].astype(jnp.int32), pair, dispatch, stride)
    arrived = exchange(leaving, "ep")
    arrived, other_gate, other_up, other_down = lax.optimization_barrier(
        (arrived, other_gate, other_up, other_down)
    )
    total = n_ep * part
    home_weights = jnp.concatenate(
        [
            lax.dynamic_slice_in_dim(group_weight, wide_offset, wide, 0),
            lax.dynamic_slice_in_dim(router_weight, wide_offset, wide, 0),
            lax.dynamic_slice_in_dim(branch_gate, wide_offset, wide, 0)[:, None],
        ],
        1,
    )
    products = jnp.dot(pair, home_weights, preferred_element_type=jnp.float32)
    expert_part = products[:, groups : groups + experts]
    home_part = jnp.concatenate(
        [products[:, :groups]]
        + [
            jnp.sum(jnp.where(expert_iota == routing[:, k : k + 1], expert_part, 0.0), 1, keepdims=True)
            for k in range(top)
        ]
        + [products[:, groups + experts :], jnp.sum(jnp.square(pair.astype(jnp.float32)), 1, keepdims=True)],
        1,
    )
    home_count = home_part.shape[1]

    gain_wide = lax.dynamic_slice_in_dim(norm_gain_ffn, wide_offset, wide, 0)[None]
    share = total // n_y
    lanes = 2 * units
    flat = jnp.pad(
        home_part.reshape(1, seq_count * home_count), ((0, 0), (0, lanes - seq_count * home_count))
    )
    high = lax.reduce_precision(flat, 8, 7)
    home_rows = jnp.concatenate([high, flat - high], 0)
    leaving = spread(arrived, gain_wide, dense_pair, home_rows, n_y, share)
    gathered = exchange(leaving, "y")
    fresh_keys = across(normed, key_weight).astype(jnp.bfloat16)
    fresh_values = across(normed, value_weight).astype(jnp.bfloat16)

    leaving, sums = run_expert(
        gathered,
        norm_gain_ffn,
        (expert_gate[0], expert_up[0], expert_down[0], other_gate, other_up, other_down),
        n_ep,
        feat,
    )
    home_sum = (sums[0] + sums[1])[: seq_count * home_count].reshape(seq_count, home_count)

    summed = exchange(leaving, "y")

    returned = exchange(merge(summed, dense_pair, n_ep, stride, part), "ep")
    inverse_two = lax.rsqrt(home_sum[:, home_count - 1 :] / width + epsilon)
    logits = home_sum[:, : home_count - 1] * inverse_two
    group_exp = jnp.exp(logits[:, :groups])
    group_iota = lax.broadcasted_iota(jnp.int32, (1, groups), 1)
    own_group = jnp.sum(
        jnp.where(group_iota == routing[:, :1] // per_group, group_exp, 0.0), 1, keepdims=True
    )
    group_prob = own_group / jnp.sum(group_exp, 1, keepdims=True)
    chosen_exp = jnp.exp(logits[:, groups : groups + top])
    route_gate = group_prob * chosen_exp / jnp.sum(chosen_exp, 1, keepdims=True)
    branch = jax.nn.sigmoid(logits[:, groups + top :])

    place = lax.broadcasted_iota(jnp.int32, (1, n_ep * stride), 1)
    block, row = place // stride, place % stride
    sequence = lax.broadcasted_iota(jnp.int32, (rows_pad, 1), 0)
    wanted = jnp.where(
        (sequence < seq_count) & (sequence // part == core), sequence % part, -seq_count
    )
    padded = jnp.pad(index, ((0, rows_pad - seq_count), (0, 0)), constant_values=-1)
    taken = [row == wanted + k * part for k in range(n_core)]
    for which in range(top):
        here = block * n_core + core == padded[:, which : which + 1]
        taken += [here & (row == seq_count + k) for k in range(n_core)]
    taken = lax.optimization_barrier(jnp.concatenate(taken, 0).astype(jnp.bfloat16))
    found = jnp.dot(
        taken, returned.reshape(n_ep * stride, feat), preferred_element_type=jnp.float32
    ).reshape(1 + top, n_core, rows_pad, feat)[:, :, :seq_count]
    mixture = [
        branch * found[0, k]
        + sum(route_gate[:, j : j + 1] * found[1 + j, k] for j in range(top))
        for k in range(n_core)
    ]
    mixture = jnp.sum(lax.all_gather(jnp.concatenate(mixture, 1), "core"), 0)
    mixed = (residual_own + lax.dynamic_slice_in_dim(mixture, core * feat, feat, 1)).astype(
        jnp.bfloat16
    )
    return (mixed, fresh_keys, fresh_values)


def solution(mesh):
    n_ep, n_tp = mesh.devices.shape
    split = Mesh(mesh.devices.reshape(n_ep, n_tp // 2, 2), ("ep", "y", "core"))
    placed = (
        P("ep", None),
        P(),
        P(TP, None),
        P(TP, None),
        P(TP, None),
        P(TP),
        P("ep", TP, None),
        P("ep", TP, None),
        P("ep"),
        P(TP, None),
        P(),
        P(),
        P(),
        P("ep", None),
        P("ep", None, TP),
        P("ep", None, TP),
        P("ep", TP, None),
        P(),
        P(TP, "ep"),
        P(TP, "ep"),
        P("ep", TP),
    )
    return jax.shard_map(
        local,
        mesh=split,
        in_specs=placed,
        out_specs=(P("ep", TP), P("ep", TP), P("ep", TP)),
        check_vma=False,
    )
```

```python
import jax
import jax.numpy as jnp
from jax import lax
from jax.experimental import pallas as pl
from jax.experimental.pallas import tpu as pltpu
from jax.sharding import Mesh, PartitionSpec as P


epsilon = 1e-06
TP = ("y", "core")


def across(left, right):
    return lax.dot_general(
        left, right, (((1,), (1,)), ((), ())), preferred_element_type=jnp.float32
    )


def attend_kernel(
    offset_ref,
    lengths_ref,
    stream_hbm,
    gain_hbm,
    query_hbm,
    keys_hbm,
    values_hbm,
    out_weight_hbm,
    terms_ref,
    normed_ref,
    stream_ref,
    gain_ref,
    query_ref,
    keys_ref,
    values_ref,
    out_weight_ref,
    sems,
):
    copies = [
        pltpu.make_async_copy(source, target, sems.at[k])
        for k, (source, target) in enumerate(
            (
                (stream_hbm, stream_ref),
                (gain_hbm, gain_ref),
                (query_hbm, query_ref),
                (keys_hbm, keys_ref),
                (values_hbm, values_ref),
                (out_weight_hbm, out_weight_ref),
            )
        )
    ]
    for copy in copies:
        copy.start()
    copies[0].wait()
    copies[1].wait()
    count, _ = stream_ref.shape
    head_size, cache_len = keys_ref.shape[1:]
    n_blocks, rows, feat = terms_ref.shape
    stream_f = stream_ref[...].astype(jnp.float32)
    inverse = lax.rsqrt(jnp.mean(stream_f * stream_f, -1, keepdims=True) + epsilon)
    normed = (stream_f * inverse * gain_ref[...].astype(jnp.float32)[None]).astype(jnp.bfloat16)
    normed_ref[...] = normed
    copies[2].wait()
    queries = across(normed, query_ref[...])
    queries = jnp.concatenate([queries, jnp.zeros((rows - count, head_size), jnp.float32)], 0)
    queries = queries.astype(jnp.bfloat16)
    row = lax.broadcasted_iota(jnp.int32, (rows, 1), 0)
    after = (
        lax.broadcasted_iota(jnp.int32, (cache_len, cache_len), 0)
        > lax.broadcasted_iota(jnp.int32, (cache_len, cache_len), 1)
    ).astype(jnp.float32)
    copies[3].wait()
    scores = jnp.zeros((rows, cache_len), jnp.float32)
    for s in range(count):
        each = jnp.dot(queries, keys_ref[s], preferred_element_type=jnp.float32)
        scores = jnp.where(row == s, each, scores)
    scores = scores * head_size ** (-0.5) + offset_ref[0]
    filled = jnp.zeros((rows, 1), jnp.int32)
    for s in range(count):
        filled = jnp.where(row == s, lengths_ref[s], filled)
    inside = lax.broadcasted_iota(jnp.int32, (rows, cache_len), 1) < filled
    tail = jnp.log1p(jnp.exp(-jnp.abs(scores)))
    log_keep = jnp.where(inside, jnp.minimum(-scores, 0.0) - tail, 0.0)
    remain = jnp.dot(
        log_keep, after, precision=lax.Precision.HIGHEST, preferred_element_type=jnp.float32
    )
    weights = jnp.where(inside, jnp.exp(jnp.minimum(scores, 0.0) - tail + remain), 0.0)
    weights = weights.astype(jnp.bfloat16)
    copies[4].wait()
    heads_out = jnp.zeros((rows, head_size), jnp.float32)
    for s in range(count):
        heads_out = jnp.where(row == s, across(weights, values_ref[s]), heads_out)
    copies[5].wait()
    terms = jnp.dot(
        heads_out.astype(jnp.bfloat16), out_weight_ref[...], preferred_element_type=jnp.float32
    ).astype(jnp.bfloat16)
    for k in range(n_blocks):
        terms_ref[k] = terms[:, k * feat : (k + 1) * feat]


def attend(stream, gain, query_w, offset, keys, values, lengths, out_weight, n_tp, rows):
    count, width = stream.shape
    whole = pl.BlockSpec(memory_space=pltpu.VMEM)
    return pl.pallas_call(
        attend_kernel,
        out_shape=(
            jax.ShapeDtypeStruct((n_tp, rows, width // n_tp), jnp.bfloat16),
            jax.ShapeDtypeStruct((count, width), jnp.bfloat16),
        ),
        in_specs=[pl.BlockSpec(memory_space=pltpu.SMEM)] * 2
        + [pl.BlockSpec(memory_space=pltpu.HBM)] * 6,
        out_specs=(whole, whole),
        scratch_shapes=[
            pltpu.VMEM(each.shape, jnp.bfloat16)
            for each in (stream, gain, query_w, keys, values, out_weight)
        ]
        + [pltpu.SemaphoreType.DMA((6,))],
        compiler_params=pltpu.CompilerParams(vmem_limit_bytes=67_043_328),
        name="attend",
    )(offset, lengths, stream, gain, query_w, keys, values, out_weight)


def pack_kernel(core_ref, pair_ref, dispatch_ref, out_ref, send_ref):
    n_ep, stride, feat = out_ref.shape
    part = pair_ref.shape[0] // 2
    pair = pair_ref[...]
    send_ref[:n_ep] = jnp.dot(dispatch_ref[...], pair, preferred_element_type=jnp.float32)
    pair = pair.astype(jnp.float32)
    mine = jnp.where(core_ref[0] == 0, pair[:part], pair[part:])
    rest = jnp.zeros((stride - 2 * part, feat), jnp.float32)
    base = jnp.concatenate([mine[:, :feat], mine[:, feat:], rest], 0)
    row = lax.broadcasted_iota(jnp.int32, (stride, 1), 0)
    for b in range(n_ep):
        block = jnp.where(row == 2 * part, send_ref[pl.ds(b, 1), :feat], base)
        block = jnp.where(row == 2 * part + 1, send_ref[pl.ds(b, 1), feat:], block)
        out_ref[b] = block.astype(jnp.bfloat16)


def pack(core, pair, dispatch, stride):
    n_ep = dispatch.shape[0]
    wide = pair.shape[1]
    whole = pl.BlockSpec(memory_space=pltpu.VMEM)
    return pl.pallas_call(
        pack_kernel,
        out_shape=jax.ShapeDtypeStruct((n_ep, stride, wide // 2), jnp.bfloat16),
        in_specs=[pl.BlockSpec(memory_space=pltpu.SMEM), whole, whole],
        out_specs=whole,
        scratch_shapes=[pltpu.VMEM((n_ep + guard, wide), jnp.float32)],
        compiler_params=pltpu.CompilerParams(vmem_limit_bytes=52 * 2**20),
        name="pack",
    )(core, pair, dispatch)


def merge_kernel(summed_ref, dense_out_ref, out_ref, act_ref, dense_ref, expert_ref, block_ref):
    n_ep, stride, feat = out_ref.shape
    n_y, _, _ = summed_ref.shape
    at_act = 2 * n_ep
    total = act_ref.shape[0] - guard
    share = total // n_y
    part = total // n_ep
    expert = jnp.zeros((at_act, feat), jnp.float32)
    for y in range(n_y):
        expert = expert + summed_ref[y, :at_act].astype(jnp.float32)
        act_ref[pl.ds(y * share, share)] = summed_ref[y, at_act:].astype(jnp.float32)[:share]
    expert_ref[:at_act] = expert
    acts = act_ref[:total].astype(jnp.bfloat16)
    for k in range(2):
        dense_ref[k, :total] = jnp.dot(
            acts, dense_out_ref[k, :, 2 * feat :], preferred_element_type=jnp.float32
        )
    block_ref[...] = jnp.zeros_like(block_ref)
    for b in range(n_ep):
        for k in range(2):
            block_ref[b, pl.ds(k * part, part)] = dense_ref[k, pl.ds(b * part, part)]
            block_ref[b, pl.ds(2 * part + k, 1)] = expert_ref[pl.ds(k * n_ep + b, 1)]
    out_ref[...] = block_ref[:, :stride].astype(jnp.bfloat16)


def merge(summed, dense_pair, n_ep, stride, part):
    feat = summed.shape[2]
    total = n_ep * part
    whole = pl.BlockSpec(memory_space=pltpu.VMEM)
    return pl.pallas_call(
        merge_kernel,
        out_shape=jax.ShapeDtypeStruct((n_ep, stride, feat), jnp.bfloat16),
        in_specs=[whole, whole],
        out_specs=whole,
        scratch_shapes=[
            pltpu.VMEM((total + guard, feat), jnp.float32),
            pltpu.VMEM((2, total + guard, feat), jnp.float32),
            pltpu.VMEM((2 * n_ep + guard, feat), jnp.float32),
            pltpu.VMEM((n_ep, stride + guard, feat), jnp.float32),
        ],
        compiler_params=pltpu.CompilerParams(vmem_limit_bytes=52 * 2**20),
        name="merge",
    )(summed, dense_pair)


def spread_kernel(arrived_ref, gain_ref, dense_in_ref, home_ref, out_ref, wide_ref, rows_ref, block_ref):
    n_ep, stride, feat = arrived_ref.shape
    n_y, rows_out, lanes = out_ref.shape
    at_expert = rows_out - n_ep
    share = at_expert - 4
    total = n_y * share
    part = total // n_ep
    wide_ref[:, :stride] = arrived_ref[...].astype(jnp.float32)
    for b in range(n_ep):
        for k in range(2):
            rows_ref[k, pl.ds(b * part, part)] = wide_ref[b, pl.ds(k * part, part)]
            rows_ref[k, pl.ds(total + b, 1)] = wide_ref[b, pl.ds(2 * part + k, 1)]
    products = jnp.zeros((total, lanes), jnp.float32)
    squares = jnp.zeros((total, 1), jnp.float32)
    for k in range(2):
        rows = rows_ref[k, :total]
        squares = squares + jnp.sum(rows * rows, 1, keepdims=True)
        gain = gain_ref[:, k * feat : (k + 1) * feat].astype(jnp.float32)
        products = products + jnp.dot(
            (rows * gain).astype(jnp.bfloat16),
            dense_in_ref[k, :, :lanes],
            preferred_element_type=jnp.float32,
        )
        picked = rows_ref[k, pl.ds(total, n_ep)].astype(jnp.bfloat16)
        for y in range(n_y):
            out_ref[y, at_expert:, k * feat : (k + 1) * feat] = picked
    diagonal = lax.broadcasted_iota(jnp.int32, (share, lanes), 0) == lax.broadcasted_iota(
        jnp.int32, (share, lanes), 1
    )
    for y in range(n_y):
        part_squares = squares[y * share : (y + 1) * share]
        line = jnp.sum(jnp.where(diagonal, part_squares, 0.0), 0, keepdims=True)
        high = line.astype(jnp.bfloat16).astype(jnp.float32)
        block_ref[y, pl.ds(0, share)] = products[y * share : (y + 1) * share]
        block_ref[y, pl.ds(share, 2)] = home_ref[...]
        block_ref[y, pl.ds(share + 2, 1)] = high
        block_ref[y, pl.ds(share + 3, 1)] = line - high
        out_ref[y, :at_expert] = block_ref[y, :at_expert].astype(jnp.bfloat16)


def spread(arrived, gain, dense_in, home, n_y, share):
    n_ep, stride, feat = arrived.shape
    lanes = home.shape[1]
    whole = pl.BlockSpec(memory_space=pltpu.VMEM)
    return pl.pallas_call(
        spread_kernel,
        out_shape=jax.ShapeDtypeStruct((n_y, share + 4 + n_ep, lanes), jnp.bfloat16),
        in_specs=[whole] * 4,
        out_specs=whole,
        scratch_shapes=[
            pltpu.VMEM((n_ep, stride + guard, feat), jnp.float32),
            pltpu.VMEM((2, n_y * share + n_ep + guard, feat), jnp.float32),
            pltpu.VMEM((n_y, share + 4 + guard, lanes), jnp.float32),
        ],
        compiler_params=pltpu.CompilerParams(vmem_limit_bytes=52 * 2**20),
        name="spread",
    )(arrived, gain, dense_in, home)


guard = 8


def silu(value):
    return value * jax.nn.sigmoid(value)


def expert_kernel(
    gathered_ref,
    gain_ref,
    gate_hbm,
    up_hbm,
    down_hbm,
    other_gate_hbm,
    other_up_hbm,
    other_down_hbm,
    out_ref,
    home_ref,
    hidden_ref,
    gate_ref,
    up_ref,
    down_ref,
    other_gate_ref,
    other_up_ref,
    other_down_ref,
    sems,
):
    copies = [
        pltpu.make_async_copy(source, target, sems.at[k])
        for k, (source, target) in enumerate(
            (
                (gate_hbm, gate_ref),
                (up_hbm, up_ref),
                (other_gate_hbm, other_gate_ref),
                (other_up_hbm, other_up_ref),
                (down_hbm, down_ref),
                (other_down_hbm, other_down_ref),
            )
        )
    ]
    for copy in copies:
        copy.start()
    n_y, rows_in, lanes = gathered_ref.shape
    n_rows, width = hidden_ref.shape
    feat = out_ref.shape[2]
    units = lanes // 2
    at_expert = rows_in - n_rows
    share = at_expert - 4

    both = gathered_ref[0, :at_expert].astype(jnp.float32)
    for k in range(1, n_y):
        both = both + gathered_ref[k, :at_expert].astype(jnp.float32)
    home_ref[...] = both[share:]
    squares = both[share + 2 : share + 3] + both[share + 3 : share + 4]
    diagonal = lax.broadcasted_iota(jnp.int32, (at_expert, lanes), 0) == lax.broadcasted_iota(
        jnp.int32, (at_expert, lanes), 1
    )
    column = jnp.sum(jnp.where(diagonal, squares, 0.0), 1, keepdims=True)
    both = both * lax.rsqrt(column / width + epsilon)
    act = (silu(both[:, :units]) * both[:, units:]).astype(jnp.bfloat16)
    for k in range(n_y):
        out_ref[k, 2 * n_rows :] = act

    squares = jnp.zeros((n_rows, 1), jnp.float32)
    for k in range(n_y):
        rows = gathered_ref[k, at_expert:].astype(jnp.float32)
        squares = squares + jnp.sum(rows * rows, 1, keepdims=True)
    inverse = lax.rsqrt(squares / width + epsilon)
    for k in range(n_y):
        rows = gathered_ref[k, at_expert:].astype(jnp.float32)
        gain = gain_ref[pl.ds(k * lanes, lanes)].astype(jnp.float32)[None]
        hidden_ref[:, k * lanes : (k + 1) * lanes] = (rows * inverse * gain).astype(jnp.bfloat16)
    hidden_in = hidden_ref[...]
    acts = []
    for k, (gate_w, up_w) in enumerate(((gate_ref, up_ref), (other_gate_ref, other_up_ref))):
        copies[2 * k].wait()
        gate = jnp.dot(hidden_in, gate_w[...], preferred_element_type=jnp.float32)
        copies[2 * k + 1].wait()
        up = jnp.dot(hidden_in, up_w[...], preferred_element_type=jnp.float32)
        acts.append((silu(gate) * up).astype(jnp.bfloat16))
    copies[4].wait()
    copies[5].wait()
    for k in range(n_y):
        columns = slice(k * lanes, (k + 1) * lanes)
        terms = jnp.dot(acts[0], down_ref[:, columns], preferred_element_type=jnp.float32)
        terms = terms + jnp.dot(
            acts[1], other_down_ref[:, columns], preferred_element_type=jnp.float32
        )
        terms = terms.astype(jnp.bfloat16)
        out_ref[k, :n_rows] = terms[:, :feat]
        out_ref[k, n_rows : 2 * n_rows] = terms[:, feat:]


def run_expert(gathered, gain, weights, n_rows, feat):
    n_y, rows_in, lanes = gathered.shape
    at_expert = rows_in - n_rows
    whole = pl.BlockSpec(memory_space=pltpu.VMEM)
    return pl.pallas_call(
        expert_kernel,
        out_shape=(
            jax.ShapeDtypeStruct((n_y, 2 * n_rows + at_expert, feat), jnp.bfloat16),
            jax.ShapeDtypeStruct((4, lanes), jnp.float32),
        ),
        in_specs=[whole, whole] + [pl.BlockSpec(memory_space=pltpu.HBM)] * 6,
        out_specs=(whole, whole),
        scratch_shapes=[pltpu.VMEM((n_rows, gain.shape[0]), jnp.bfloat16)]
        + [pltpu.VMEM(weights[k].shape, jnp.bfloat16) for k in range(6)]
        + [pltpu.SemaphoreType.DMA((6,))],
        compiler_params=pltpu.CompilerParams(vmem_limit_bytes=52 * 2**20),
        name="expert",
    )(gathered, gain, *weights)


def exchange(array, axis):
    return lax.all_to_all(array, axis, 0, 0, tiled=True)


def round_up(count, unit=8):
    return -(-count // unit) * unit


def sum_lead(array):
    return jnp.sum(array.astype(jnp.float32), axis=0)


def local(
    stream,
    norm_gain_mix,
    query_weight,
    key_weight,
    value_weight,
    score_offset,
    cache_keys,
    cache_values,
    lengths,
    out_weight,
    norm_gain_ffn,
    group_weight,
    router_weight,
    routing,
    expert_gate,
    expert_up,
    expert_down,
    branch_gate,
    dense_gate,
    dense_up,
    dense_down,
):
    seq_count = stream.shape[0]
    width = stream.shape[1]
    n_tp = lax.axis_size(TP)
    n_ep = lax.axis_size("ep")
    n_y = lax.axis_size("y")
    n_core = lax.axis_size("core")
    core = lax.axis_index("core")
    feat = width // n_tp
    offset = lax.axis_index(TP) * feat
    wide = n_core * feat
    wide_offset = lax.axis_index("y") * wide

    swap = [(0, 1), (1, 0)]
    other_gate = lax.ppermute(expert_gate[0], "core", swap)
    other_up = lax.ppermute(expert_up[0], "core", swap)
    other_down = lax.ppermute(expert_down[0], "core", swap)
    dense_pair = lax.all_gather(
        jnp.concatenate([dense_gate, dense_up, dense_down], 1), "core"
    )
    units = dense_gate.shape[1]
    rows_pad = round_up(seq_count)

    stream_own = lax.optimization_barrier(
        lax.dynamic_slice_in_dim(stream, offset, feat, 1).astype(jnp.float32)
    )
    terms, normed = attend(
        stream,
        norm_gain_mix,
        query_weight,
        score_offset,
        cache_keys,
        cache_values,
        lengths,
        out_weight,
        n_tp,
        rows_pad,
    )
    attn = sum_lead(exchange(terms, TP))[:seq_count]

    residual = (
        stream_own
        + attn.astype(jnp.bfloat16).astype(jnp.float32)
    ).astype(jnp.bfloat16)
    residual_own = residual.astype(jnp.float32)
    pair = lax.all_gather(residual, "core", axis=1, tiled=True)

    experts = router_weight.shape[1]
    groups = group_weight.shape[1]
    per_group = experts // groups
    top = routing.shape[1]
    cap = 2 * ((seq_count + experts - 1) // experts)
    expert_iota = lax.broadcasted_iota(jnp.int32, (1, experts), 1)
    pair_expert = routing.reshape(seq_count * top)
    onehot = (pair_expert[:, None] == expert_iota).astype(jnp.int32)
    before = jnp.cumsum(onehot, 0) - onehot
    slot = jnp.sum(before * onehot, 1)
    index = (pair_expert * cap + slot).reshape(seq_count, top)
    slot_iota = n_core * lax.broadcasted_iota(jnp.int32, (experts, 1, 1), 0) + core
    dispatch = jnp.sum((index[None, :, :] == slot_iota).astype(jnp.int32), 2).astype(jnp.bfloat16)

    part = seq_count // n_core
    stride = round_up(seq_count + n_core)
    leaving = pack(core[None].astype(jnp.int32), pair, dispatch, stride)
    arrived = exchange(leaving, "ep")
    arrived, other_gate, other_up, other_down = lax.optimization_barrier(
        (arrived, other_gate, other_up, other_down)
    )
    total = n_ep * part
    home_weights = jnp.concatenate(
        [
            lax.dynamic_slice_in_dim(group_weight, wide_offset, wide, 0),
            lax.dynamic_slice_in_dim(router_weight, wide_offset, wide, 0),
            lax.dynamic_slice_in_dim(branch_gate, wide_offset, wide, 0)[:, None],
        ],
        1,
    )
    products = jnp.dot(pair, home_weights, preferred_element_type=jnp.float32)
    expert_part = products[:, groups : groups + experts]
    home_part = jnp.concatenate(
        [products[:, :groups]]
        + [
            jnp.sum(jnp.where(expert_iota == routing[:, k : k + 1], expert_part, 0.0), 1, keepdims=True)
            for k in range(top)
        ]
        + [products[:, groups + experts :], jnp.sum(jnp.square(pair.astype(jnp.float32)), 1, keepdims=True)],
        1,
    )
    home_count = home_part.shape[1]

    gain_wide = lax.dynamic_slice_in_dim(norm_gain_ffn, wide_offset, wide, 0)[None]
    share = total // n_y
    lanes = 2 * units
    flat = jnp.pad(
        home_part.reshape(1, seq_count * home_count), ((0, 0), (0, lanes - seq_count * home_count))
    )
    high = lax.reduce_precision(flat, 8, 7)
    home_rows = jnp.concatenate([high, flat - high], 0)
    leaving = spread(arrived, gain_wide, dense_pair, home_rows, n_y, share)
    gathered = exchange(leaving, "y")
    fresh_keys = across(normed, key_weight).astype(jnp.bfloat16)
    fresh_values = across(normed, value_weight).astype(jnp.bfloat16)

    leaving, sums = run_expert(
        gathered,
        norm_gain_ffn,
        (expert_gate[0], expert_up[0], expert_down[0], other_gate, other_up, other_down),
        n_ep,
        feat,
    )
    home_sum = (sums[0] + sums[1])[: seq_count * home_count].reshape(seq_count, home_count)

    summed = exchange(leaving, "y")

    returned = exchange(merge(summed, dense_pair, n_ep, stride, part), "ep")
    inverse_two = lax.rsqrt(home_sum[:, home_count - 1 :] / width + epsilon)
    logits = home_sum[:, : home_count - 1] * inverse_two
    group_exp = jnp.exp(logits[:, :groups])
    group_iota = lax.broadcasted_iota(jnp.int32, (1, groups), 1)
    own_group = jnp.sum(
        jnp.where(group_iota == routing[:, :1] // per_group, group_exp, 0.0), 1, keepdims=True
    )
    group_prob = own_group / jnp.sum(group_exp, 1, keepdims=True)
    chosen_exp = jnp.exp(logits[:, groups : groups + top])
    route_gate = group_prob * chosen_exp / jnp.sum(chosen_exp, 1, keepdims=True)
    branch = jax.nn.sigmoid(logits[:, groups + top :])

    place = lax.broadcasted_iota(jnp.int32, (1, n_ep * stride), 1)
    block, row = place // stride, place % stride
    sequence = lax.broadcasted_iota(jnp.int32, (rows_pad, 1), 0)
    wanted = jnp.where(
        (sequence < seq_count) & (sequence // part == core), sequence % part, -seq_count
    )
    padded = jnp.pad(index, ((0, rows_pad - seq_count), (0, 0)), constant_values=-1)
    taken = [row == wanted + k * part for k in range(n_core)]
    for which in range(top):
        here = block * n_core + core == padded[:, which : which + 1]
        taken += [here & (row == seq_count + k) for k in range(n_core)]
    taken = lax.optimization_barrier(jnp.concatenate(taken, 0).astype(jnp.bfloat16))
    found = jnp.dot(
        taken, returned.reshape(n_ep * stride, feat), preferred_element_type=jnp.float32
    ).reshape(1 + top, n_core, rows_pad, feat)[:, :, :seq_count]
    mixture = [
        branch * found[0, k]
        + sum(route_gate[:, j : j + 1] * found[1 + j, k] for j in range(top))
        for k in range(n_core)
    ]
    mixture = jnp.sum(lax.all_gather(jnp.concatenate(mixture, 1), "core"), 0)
    mixed = (residual_own + lax.dynamic_slice_in_dim(mixture, core * feat, feat, 1)).astype(
        jnp.bfloat16
    )
    return (mixed, fresh_keys, fresh_values)


def solution(mesh):
    n_ep, n_tp = mesh.devices.shape
    split = Mesh(mesh.devices.reshape(n_ep, n_tp // 2, 2), ("ep", "y", "core"))
    placed = (
        P("ep", None),
        P(),
        P(TP, None),
        P(TP, None),
        P(TP, None),
        P(TP),
        P("ep", TP, None),
        P("ep", TP, None),
        P("ep"),
        P(TP, None),
        P(),
        P(),
        P(),
        P("ep", None),
        P("ep", None, TP),
        P("ep", None, TP),
        P("ep", TP, None),
        P(),
        P(TP, "ep"),
        P(TP, "ep"),
        P("ep", TP),
    )
    return jax.shard_map(
        local,
        mesh=split,
        in_specs=placed,
        out_specs=(P("ep", TP), P("ep", TP), P("ep", TP)),
        check_vma=False,
    )
```
